32 devices in a mesh: sp: 8 (over z, x), tp: 4 (over y, core).
Axes of the slice: x: 2, y: 2, z: 4, core: 2. Of those that a mesh axis runs over, the one named last changes fastest.
Arguments:
- out_gate: bfloat16 [4096, 1536], P('sp', 'tp'), may hold values from -6 to 6
- in_gate: bfloat16 [4096, 1536], P('sp', 'tp'), may hold values from -6 to 6
- conv_values: bfloat16 [4096, 1536], P('sp', 'tp'), may hold values from -6 to 6
- conv_taps: float32 [3, 1536], P(None, 'tp'), may hold values from -3 to 3
- mix_gain: float32 [1536], replicated, may hold values from 0.1 to 1.9
- out_proj: bfloat16 [1536, 2048], replicated, may hold values from -0.15625 to 0.15625
- residual: bfloat16 [4096, 2048], P(('sp', 'tp')), may hold values from -6 to 6
- ffn_gain: float32 [2048], replicated, may hold values from 0.1 to 1.9
- routes: int32 [4096, 6], P(('sp', 'tp')), may hold values from 0 to 31, all different within a row; in each aligned block of 128 rows (0 to 127, 128 to 255, ...) at most 32 rows name the same one
- route_weights: float32 [4096, 6], P(('sp', 'tp')), may hold values from 0.05 to 1
- shared_gate: bfloat16 [2048, 512], replicated, may hold values from -0.125 to 0.125
- shared_up: bfloat16 [2048, 512], replicated, may hold values from -0.125 to 0.125
- shared_down: bfloat16 [512, 2048], replicated, may hold values from -0.25 to 0.25
- expert_gate: bfloat16 [32, 2048, 512], P(('sp', 'tp')), may hold values from -0.125 to 0.125
- expert_up: bfloat16 [32, 2048, 512], P(('sp', 'tp')), may hold values from -0.125 to 0.125
- expert_down: bfloat16 [32, 512, 2048], P(('sp', 'tp')), may hold values from -0.25 to 0.25
Outputs:
- layer_out: bfloat16 [4096, 2048], P(('sp', 'tp'))
The draws below stay inside these ranges and needn't reach their ends.
Inputs may be any that keep to these rules, and one draw needn't show every extreme that they name: `routes`: each row names 6 different experts. Within the rows of one device (aligned blocks of 128 rows) no expert is named more than 32 times, a bound that some block reaches.
All inputs are finite; a program needn't handle non-finite values.
Results may differ from the reference program's by a relative error of at most 0.0065.
Values may be sent and summed in bfloat16 or wider, within the bound.
No kernel may reach another device: no remote copies, remote signals or barrier semaphores. Data moves between devices by JAX's collectives and lax.ppermute only.
A program may use at most 128 MiB of HBM per device.

```python
import math
import jax
import jax.numpy as jnp
import numpy as np
from jax import lax

D = 2048
DC = 1536
KERNEL = 3
FF_E = 512
FS = 512
TOP = 6
ROWS_DEV = 128
TOKENS = 4096
EXPERTS = 32
CAP = 32
N_SP = 8
N_TP = 4


def levels(key, shape, shards, smallest, largest):
    level = 1.0
    for axis_at, parts in shards:
        steps = jax.random.uniform(jax.random.fold_in(jax.random.fold_in(key, 6), axis_at), (parts,), jnp.float32, smallest / len(shards), largest / len(shards))
        level = level * jnp.repeat(jnp.exp(steps), shape[axis_at] // parts).reshape((-1,) + (1,) * (len(shape) - 1 - axis_at))
    return level


def deal_out(stream_key, own, number, rows, number_of, top, limit, slope):
    order = jax.random.permutation(stream_key, number_of)
    packed, common = portions_of(number_of, rows * top, limit, slope, True), portions_of(number_of, rows * top, limit, slope, False)
    places = jnp.arange(number_of)

    def named(sizes, offset_by):
        used = int((sizes > 0).sum())
        fixed = max(1, used // 4)
        passed = fixed + (places - fixed + offset_by * (used - fixed)) % max(1, number_of - fixed)
        return jnp.zeros((number_of,), jnp.int32).at[order[jnp.where(places < fixed, places, passed)]].set(jnp.asarray(sizes, jnp.int32))

    sizes = jnp.where(number % 4 == 0, named(packed, number // 4), named(common, number - number // 4 - 1))
    mixed = jax.random.permutation(jax.random.fold_in(own, 3), number_of)
    source_of, taker = mixed[0:number_of // 2 * 2:2], mixed[1:number_of // 2 * 2:2]
    margin = jnp.minimum(sizes[source_of] - 1, limit - sizes[taker]) // 2
    margin = jnp.where((source_of == order[0]) | (taker == order[0]) | (sizes[taker] == 0), 0, jnp.maximum(margin, 0))
    passed = jax.random.randint(jax.random.fold_in(own, 4), (number_of // 2,), 0, 1 << 20) % (margin + 1)
    sizes = sizes.at[source_of].add(-passed).at[taker].add(passed)
    labels = jnp.searchsorted(jnp.cumsum(sizes), jnp.arange(rows * top), side="right").astype(jnp.int32)
    listing = labels.reshape(top, rows).T
    listing = listing[jax.random.permutation(jax.random.fold_in(own, 1), rows)]
    offset_by = jax.random.randint(jax.random.fold_in(own, 2), (rows, 1), 0, top)
    return jnp.take_along_axis(listing, (jnp.arange(top)[None, :] + offset_by) % top, axis=1)


def portions_of(count, total, reach, slope, full):
    portions = [(1 << 20) // math.isqrt(rank ** slope) + 1 for rank in range(1, count + 1)]
    largest = reach if full else min(reach, max(-(-total // count), total * portions[0] // sum(portions)))
    least = 1 if total - largest >= count - 1 else 0
    given, surplus = [largest] + [least] * (count - 1), total - largest - least * (count - 1)
    while surplus > 0:
        movable = [i for i in range(1, count) if given[i] < largest] or [i for i in range(1, count) if given[i] < reach]
        whole, remaining = sum([portions[i] for i in movable]), surplus
        for i in movable:
            addition = min(reach - given[i], max(1, remaining * portions[i] // whole), surplus)
            given[i] = given[i] + addition
            surplus = surplus - addition
    return np.array(given)


def gaussian(own_key, shape, deviation, limit, split=(), kind=jnp.bfloat16):
    values = jax.random.normal(own_key, shape, jnp.float32) * deviation
    if len(split) > 0:
        values = levels(own_key, shape, split, -0.22, 0.18) * values
    return jnp.clip(values, min=-limit, max=limit).astype(kind)


def setup_inputs(seed: int = 0) -> dict:
    splits = jax.random.split(jax.random.key(seed), 17)
    out_gate = gaussian(splits[0], (TOKENS, DC), 1.0, 6.0, ((0, 8), (1, 4)))
    in_gate = gaussian(splits[1], (TOKENS, DC), 1.0, 6.0, ((0, 8), (1, 4)))
    conv_values = gaussian(splits[2], (TOKENS, DC), 1.0, 6.0, ((0, 8), (1, 4)))
    conv_taps = gaussian(splits[3], (KERNEL, DC), 0.6, 3.0, ((1, 4),), jnp.float32)
    mix_gain = jnp.clip(1.0 + 0.18 * jax.random.normal(splits[4], (DC,), jnp.float32), 0.1, 1.9)
    out_proj = gaussian(splits[5], (DC, D), DC ** -0.5, 0.15625)
    residual = gaussian(splits[6], (TOKENS, D), 1.0, 6.0, ((0, 32),))
    ffn_gain = jnp.clip(1.0 + 0.18 * jax.random.normal(splits[7], (D,), jnp.float32), 0.1, 1.9)
    routes_keys = jax.random.split(jax.random.fold_in(splits[8], 1), TOKENS // ROWS_DEV)
    routes_turns = jax.random.permutation(jax.random.fold_in(splits[8], 3), TOKENS // ROWS_DEV)
    routes = jax.vmap(lambda own, number: deal_out(jax.random.fold_in(splits[8], 2), own, number, ROWS_DEV, EXPERTS, TOP, CAP, 2))(routes_keys, routes_turns).reshape((TOKENS, TOP))
    route_weights = jnp.clip(jnp.exp(math.log(1.0) - 2.9957323 * jax.random.uniform(splits[9], (TOKENS, TOP), jnp.float32) ** levels(splits[9], (TOKENS, TOP), ((0, 32),), -0.2, 0.2)), 0.05, 1.0)
    shared_gate = gaussian(splits[10], (D, FS), D ** -0.5, 0.125)
    shared_up = gaussian(splits[11], (D, FS), D ** -0.5, 0.125)
    shared_down = gaussian(splits[12], (FS, D), FS ** -0.5, 0.25)
    expert_gate = gaussian(splits[13], (EXPERTS, D, FF_E), D ** -0.5, 0.125, ((0, 32),))
    expert_up = gaussian(splits[14], (EXPERTS, D, FF_E), D ** -0.5, 0.125, ((0, 32),))
    expert_down = gaussian(splits[15], (EXPERTS, FF_E, D), FF_E ** -0.5, 0.25, ((0, 32),))
    return dict(out_gate=out_gate, in_gate=in_gate, conv_values=conv_values, conv_taps=conv_taps, mix_gain=mix_gain, out_proj=out_proj, residual=residual, ffn_gain=ffn_gain, routes=routes, route_weights=route_weights, shared_gate=shared_gate, shared_up=shared_up, shared_down=shared_down, expert_gate=expert_gate, expert_up=expert_up, expert_down=expert_down)


def project_norm(conv_out, mix_gain, out_proj):
    values = conv_out.astype(jnp.float32)
    inverse = lax.rsqrt(lax.optimization_barrier(jnp.mean(values * values, axis=-1)) + 1e-06)
    scaled = (values * mix_gain).astype(jnp.bfloat16)
    return jnp.dot(scaled, out_proj, preferred_element_type=jnp.float32) * inverse[:, None]

def ffn_input(stream, ffn_gain):
    inverse = lax.rsqrt(lax.optimization_barrier(jnp.mean(stream * stream, axis=-1, keepdims=True)) + 1e-06)
    return (stream * inverse * ffn_gain).astype(jnp.bfloat16)

def swiglu_hidden(row_block, weight_gate, weight_up):
    gate_part = jnp.dot(row_block, weight_gate, preferred_element_type=jnp.float32)
    up_part = jnp.dot(row_block, weight_up, preferred_element_type=jnp.float32)
    return (jax.nn.silu(gate_part) * up_part).astype(jnp.bfloat16)

def reference(out_gate, in_gate, conv_values, conv_taps, mix_gain, out_proj, residual, ffn_gain, routes, route_weights, shared_gate, shared_up, shared_down, expert_gate, expert_up, expert_down):
    mixed_in = in_gate.astype(jnp.float32) * conv_values.astype(jnp.float32)
    taps_count = conv_taps.shape[0]
    length = mixed_in.shape[0]
    extended = jnp.concatenate([jnp.zeros((taps_count - 1, mixed_in.shape[1]), jnp.float32), mixed_in], axis=0)
    filtered = conv_taps[0] * extended[0:length]
    for offset in range(1, taps_count):
        filtered = filtered + conv_taps[offset] * extended[offset:offset + length]
    conv_out = (out_gate.astype(jnp.float32) * filtered).astype(jnp.bfloat16)
    stream = residual.astype(jnp.float32) + project_norm(conv_out, mix_gain, out_proj)
    normed = ffn_input(stream, ffn_gain)
    shared_result = jnp.dot(swiglu_hidden(normed, shared_gate, shared_up), shared_down, preferred_element_type=jnp.float32)
    top_count = routes.shape[1]
    token_count = routes.shape[0]
    model_width = normed.shape[1]
    flat_ids = routes.reshape(-1).astype(jnp.int32)
    gate_values = route_weights / lax.optimization_barrier(jnp.sum(route_weights, axis=1, keepdims=True)) * 2.5
    flat_gates = gate_values.reshape(-1)
    sort_order = jnp.argsort(flat_ids, stable=True).astype(jnp.int32)
    sorted_ids = flat_ids[sort_order]
    counts = jnp.bincount(flat_ids, length=EXPERTS).astype(jnp.int32)
    starts = (jnp.cumsum(counts) - counts).astype(jnp.int32)
    slot_rank = jnp.arange(flat_ids.shape[0], dtype=jnp.int32) - starts[sorted_ids]
    most_rows = N_SP * N_TP * CAP
    slot_index = (sorted_ids * most_rows + slot_rank).astype(jnp.int32)
    row_of = (sort_order // top_count).astype(jnp.int32)
    slot_rows = jnp.full((EXPERTS * most_rows,), token_count, jnp.int32).at[slot_index].set(row_of)
    slot_gates = jnp.zeros((EXPERTS * most_rows,), jnp.float32).at[slot_index].set(flat_gates[sort_order])
    padded = jnp.concatenate([normed, jnp.zeros((1, model_width), jnp.bfloat16)], axis=0)

    def add_expert(running, inputs):
        row_index, gate_slots, weight_gate, weight_up, weight_down = inputs
        picked = padded[row_index]
        hidden = swiglu_hidden(picked, weight_gate, weight_up)
        result = jnp.dot(hidden, weight_down, preferred_element_type=jnp.float32).astype(jnp.bfloat16)
        return (running.at[row_index].add(result.astype(jnp.float32) * gate_slots[:, None]), None)
    running = jnp.zeros((token_count + 1, model_width), jnp.float32)
    running, _ = lax.scan(add_expert, running, (slot_rows.reshape(EXPERTS, most_rows), slot_gates.reshape(EXPERTS, most_rows), expert_gate, expert_up, expert_down))
    routed = running[:token_count]
    return (stream + shared_result + routed).astype(jnp.bfloat16)
```

```python
import jax
import jax.numpy as jnp
from jax import lax
from jax.sharding import Mesh, PartitionSpec as P

PLANE = ("x", "tp")
SEQ = ("z", "x")


def from_behind(block, distance):
    count = lax.axis_size(SEQ)
    route = [(i - distance, i) for i in range(distance, count)]
    return lax.ppermute(block, SEQ, route)


def project_norm(conv_out, mix_gain, out_proj):
    values = conv_out.astype(jnp.float32)
    inverse = lax.rsqrt(jnp.mean(values * values, axis=-1) + 1e-06)
    scaled = (values * mix_gain).astype(jnp.bfloat16)
    return jnp.dot(scaled, out_proj, preferred_element_type=jnp.float32) * inverse[:, None]


def swiglu_hidden(row_block, weight_gate, weight_up):
    gate_part = jnp.dot(row_block, weight_gate, preferred_element_type=jnp.float32)
    up_part = jnp.dot(row_block, weight_up, preferred_element_type=jnp.float32)
    return (jax.nn.silu(gate_part) * up_part).astype(jnp.bfloat16)


def flips(count, distance):
    return [(i, i ^ distance) for i in range(count)]


def gather_line(own, count):
    if count != 4:
        return [own] + [lax.ppermute(own, "z", flips(count, j)) for j in range(1, count)]
    sides, middle = flips(4, 1), [(1, 2), (2, 1)]
    near = lax.ppermute(own, "z", sides)
    across = lax.ppermute(own, "z", middle)
    across_far = lax.ppermute(near, "z", middle)
    side_far = lax.ppermute(across, "z", sides)
    side_end = lax.ppermute(across_far, "z", sides)
    return [own, near, across_far + side_far, across + side_end]


def exchange(block):
    return lax.all_to_all(block, PLANE, split_axis=0, concat_axis=0, tiled=True)


def body(
    out_gate,
    in_gate,
    conv_values,
    conv_taps,
    mix_gain,
    out_proj,
    residual,
    ffn_gain,
    routes,
    route_weights,
    shared_gate,
    shared_up,
    shared_down,
    expert_gate,
    expert_up,
    expert_down,
):
    bf16, f32 = jnp.bfloat16, jnp.float32
    z_count, tp_count = lax.axis_size("z"), lax.axis_size("tp")
    plane_count = lax.axis_size("x") * tp_count
    experts_total = z_count * plane_count
    z_index = lax.axis_index("z")

    row_count, top_count = routes.shape
    capacity = max(2, 4 * row_count * top_count // (3 * experts_total))
    gate_values = route_weights / jnp.sum(route_weights, axis=1, keepdims=True) * 2.5
    experts = jnp.arange(experts_total, dtype=jnp.int32)
    hits = routes.T[:, None, :] == experts[None, :, None]
    named = jnp.any(hits, axis=0)
    gates_of = jnp.sum(jnp.where(hits, gate_values.T[:, None, :], 0.0), axis=0)
    steps = jnp.arange(row_count, dtype=jnp.int32)
    earlier = (steps[:, None] < steps[None, :]).astype(bf16)
    rank = jnp.dot(named.astype(bf16), earlier, preferred_element_type=f32)
    rank = jnp.where(named, rank, -1.0)
    table = jnp.stack([rank, gates_of]).reshape(2, z_count, plane_count, row_count)

    def for_plane(distance):
        part = lax.dynamic_index_in_dim(table, z_index ^ distance, axis=1, keepdims=False)
        if distance == 0:
            return part
        return lax.ppermute(part, "z", flips(z_count, distance))

    tables = [for_plane(j) for j in range(z_count)]

    mixed_in = in_gate.astype(f32) * conv_values.astype(f32)
    taps_count = conv_taps.shape[0]
    length = mixed_in.shape[0]
    before = from_behind(mixed_in[length - (taps_count - 1) :], 1)
    extended = jnp.concatenate([before, mixed_in], axis=0)
    filtered = conv_taps[0] * extended[0:length]
    for offset in range(1, taps_count):
        filtered = filtered + conv_taps[offset] * extended[offset : offset + length]
    conv_out = (out_gate.astype(f32) * filtered).astype(bf16)
    token_rows = lax.all_to_all(conv_out, "tp", split_axis=0, concat_axis=1, tiled=True)
    stream = residual.astype(f32) + project_norm(token_rows, mix_gain, out_proj)
    norm_inverse = lax.rsqrt(jnp.mean(stream * stream, axis=-1, keepdims=True) + 1e-06)
    normed = (stream * norm_inverse * ffn_gain).astype(bf16)

    model_width = normed.shape[1]
    slots = jnp.arange(capacity, dtype=jnp.int32).astype(f32)
    blocks = gather_line(normed, z_count)
    arrived = []
    for j in range(z_count):
        pick = (tables[j][0][:, None, :] == slots[None, :, None]).astype(bf16)
        pick = pick.reshape(plane_count * capacity, row_count)
        outgoing = jnp.dot(pick, blocks[j], preferred_element_type=f32).astype(bf16)
        arrived.append(exchange(outgoing.reshape(plane_count, capacity, model_width)))

    shared_result = jnp.dot(
        swiglu_hidden(normed, shared_gate, shared_up), shared_down, preferred_element_type=f32
    )
    base = stream + shared_result

    partial = [None] * z_count
    for j in reversed(range(z_count)):
        rows = arrived[j].reshape(plane_count * capacity, model_width)
        hidden = swiglu_hidden(rows, expert_gate[0], expert_up[0])
        result = jnp.dot(hidden, expert_down[0], preferred_element_type=f32).astype(bf16)
        returned = exchange(result.reshape(plane_count, capacity, model_width))
        returned = returned.reshape(plane_count * capacity, model_width)
        chosen = tables[j][0][:, None, :] == slots[None, :, None]
        weight = jnp.where(chosen, tables[j][1][:, None, :], 0.0)
        weight = weight.reshape(plane_count * capacity, row_count)
        high = lax.reduce_precision(weight, exponent_bits=8, mantissa_bits=7)
        low = (weight - high).astype(bf16)
        both = jnp.concatenate([high.astype(bf16), low], axis=0)
        twice = jnp.concatenate([returned, returned], axis=0)
        partial[j] = lax.dot_general(
            both, twice, (((0,), (0,)), ((), ())), preferred_element_type=f32
        )

    if z_count == 4:
        outward, middle, sides = [(0, 1), (3, 2)], [(1, 2), (2, 1)], flips(4, 1)
        far = lax.ppermute(partial[3].astype(bf16), "z", outward).astype(f32)
        mid = lax.ppermute(partial[2].astype(bf16), "z", outward).astype(f32)
        far = lax.ppermute((far + partial[2]).astype(bf16), "z", middle).astype(f32)
        mid = lax.ppermute((mid + partial[3]).astype(bf16), "z", middle).astype(f32)
        last = lax.ppermute((far + partial[1]).astype(bf16), "z", sides).astype(f32)
        routed = partial[0] + mid + last
    else:
        routed = partial[0]
        for j in range(1, z_count):
            routed = routed + lax.ppermute(partial[j].astype(bf16), "z", flips(z_count, j))
    return (base + routed).astype(bf16)


def solution(mesh):
    sp_count, tp_count = mesh.shape["sp"], mesh.shape["tp"]
    z_count = 1 << -(-(sp_count.bit_length() - 1) // 2)
    split = Mesh(
        mesh.devices.reshape(z_count, sp_count // z_count, tp_count), ("z", "x", "tp")
    )
    every = ("z", "x", "tp")
    in_specs = (
        P(SEQ, "tp"),
        P(SEQ, "tp"),
        P(SEQ, "tp"),
        P(None, "tp"),
        P(),
        P(),
        P(every, None),
        P(),
        P(every, None),
        P(every, None),
        P(),
        P(),
        P(),
        P(every, None, None),
        P(every, None, None),
        P(every, None, None),
    )
    return jax.shard_map(
        body, mesh=split, in_specs=in_specs, out_specs=P(every, None), check_vma=False
    )
```

```python
import functools

import jax
import jax.numpy as jnp
from jax import lax
from jax.experimental import pallas as pl
from jax.experimental.pallas import tpu as pltpu
from jax.sharding import Mesh, PartitionSpec as P

PLANE = ("x", "tp")
SEQ = ("z", "x")
BF16, F32 = jnp.bfloat16, jnp.float32


def flips(count, distance):
    return [(i, i ^ distance) for i in range(count)]


def from_behind(block, distance):
    count = lax.axis_size(SEQ)
    route = [(i - distance, i) for i in range(distance, count)]
    return lax.ppermute(block, SEQ, route)


def cost(flops, arrays):
    size = sum(a.size * a.dtype.itemsize for a in arrays)
    return pl.CostEstimate(flops=flops, bytes_accessed=size, transcendentals=0)


def filter_kernel(parts, taps_count, me_ref, gate_ref, in_ref, val_ref, taps_ref, halo_ref, *rest):
    outs, scratch = rest[:parts], rest[parts]
    length = val_ref.shape[0]
    rows = length // parts
    back = taps_count - 1
    scratch[0:8] = jnp.zeros((8, scratch.shape[1]), F32)
    scratch[8 - back : 8] = halo_ref[...]
    scratch[8:] = in_ref[...].astype(F32) * val_ref[...].astype(F32)
    me = me_ref[0]
    for k in range(parts):
        start = pl.multiple_of((me ^ k) * rows, 16)
        window = scratch[pl.ds(start, rows + 8)]
        total = taps_ref[0:1] * window[8 - back : 8 - back + rows]
        for offset in range(1, taps_count):
            first = 8 - back + offset
            total = total + taps_ref[offset : offset + 1] * window[first : first + rows]
        outs[k][...] = (gate_ref[pl.ds(start, rows)].astype(F32) * total).astype(BF16)


def filter_rows(me, out_gate, in_gate, conv_values, conv_taps, halo, parts):
    length, channels = conv_values.shape
    out = jax.ShapeDtypeStruct((length // parts, channels), BF16)
    whole = pl.BlockSpec(memory_space=pltpu.VMEM)
    return pl.pallas_call(
        functools.partial(filter_kernel, parts, conv_taps.shape[0]),
        out_shape=[out] * parts,
        in_specs=[pl.BlockSpec(memory_space=pltpu.SMEM)] + [whole] * 5,
        out_specs=[whole] * parts,
        scratch_shapes=[pltpu.VMEM((length + 8, channels), F32)],
        cost_estimate=cost(8 * out_gate.size, [out_gate, in_gate, conv_values]),
        name="filter_rows",
    )(me, out_gate, in_gate, conv_values, conv_taps, halo)


def mix_kernel(parts, me_ref, *refs):
    pieces = refs[:parts]
    mix_gain, out_proj, residual, ffn_gain, stream_ref, normed_ref, acc, squares = refs[parts:]
    step = pl.program_id(0)

    @pl.when(step == 0)
    def _():
        acc[...] = jnp.zeros_like(acc)
        squares[...] = jnp.zeros_like(squares)

    for k in range(parts):

        @pl.when(step == k)
        def _(k=k):
            values = pieces[k][...].astype(F32)
            squares[...] += jnp.sum(values * values, axis=1, keepdims=True)
            scaled = (values * mix_gain[0]).astype(BF16)
            acc[...] += jnp.dot(scaled, out_proj[...], preferred_element_type=F32)

    @pl.when(step == parts - 1)
    def _():
        channels = parts * pieces[0].shape[1]
        inverse = lax.rsqrt(squares[...] / channels + 1e-06)
        stream = residual[...].astype(F32) + acc[...] * inverse
        stream_ref[...] = stream
        mean = jnp.mean(stream * stream, axis=1, keepdims=True)
        normed_ref[...] = (stream * lax.rsqrt(mean + 1e-06) * ffn_gain[...]).astype(BF16)


def mix_project(me, pieces, mix_gain, out_proj, residual, ffn_gain):
    parts = len(pieces)
    rows, channels = pieces[0].shape
    width = out_proj.shape[1]
    fixed = lambda shape: pl.BlockSpec(shape, lambda i, me_ref: (0,) * len(shape))
    out_shape = [
        jax.ShapeDtypeStruct((rows, width), F32),
        jax.ShapeDtypeStruct((rows, width), BF16),
    ]
    grid_spec = pltpu.PrefetchScalarGridSpec(
        num_scalar_prefetch=1,
        grid=(parts,),
        in_specs=[fixed((rows, channels))] * parts
        + [
            pl.BlockSpec((1, 1, channels), lambda i, me_ref: (me_ref[0] ^ i, 0, 0)),
            pl.BlockSpec((channels, width), lambda i, me_ref: (me_ref[0] ^ i, 0)),
            fixed((rows, width)),
            fixed((1, width)),
        ],
        out_specs=[fixed((rows, width))] * 2,
        scratch_shapes=[pltpu.VMEM((rows, width), F32), pltpu.VMEM((rows, 1), F32)],
    )
    return pl.pallas_call(
        functools.partial(mix_kernel, parts),
        out_shape=out_shape,
        grid_spec=grid_spec,
        cost_estimate=cost(2 * rows * out_proj.size, [out_proj, residual] + out_shape),
        name="mix_project",
    )(me, *pieces, mix_gain.reshape(parts, 1, channels), out_proj, residual, ffn_gain[None])


def expert_kernel(parts, *refs):
    pieces, outs = refs[:parts], refs[parts + 3 : 2 * parts + 3]
    gate_ref, up_ref, down_ref = refs[parts : parts + 3]
    rows, acc = refs[2 * parts + 3 :]
    size = pieces[0].shape[0]
    step = pl.program_id(0)

    @pl.when(step == 0)
    def _():
        for k in range(parts):
            rows[k * size : (k + 1) * size] = pieces[k][...]

    gate_part = jnp.dot(rows[...], gate_ref[0], preferred_element_type=F32)
    up_part = jnp.dot(rows[...], up_ref[0], preferred_element_type=F32)
    hidden = (gate_part / (1.0 + jnp.exp(-gate_part)) * up_part).astype(BF16)
    term = jnp.dot(hidden, down_ref[0], preferred_element_type=F32)

    @pl.when(step == 0)
    def _():
        acc[...] = term

    @pl.when(step > 0)
    def _():
        acc[...] += term

    @pl.when(step == pl.num_programs(0) - 1)
    def _():
        for k in range(parts):
            outs[k][...] = acc[k * size : (k + 1) * size].astype(BF16)


def expert_rows(pieces, expert_gate, expert_up, expert_down):
    parts = len(pieces)
    size, width = pieces[0].shape
    hidden = expert_gate.shape[2]
    tile = min(256, hidden)
    piece = pl.BlockSpec((size, width), lambda i: (0, 0))
    out = jax.ShapeDtypeStruct((size, width), BF16)
    weights = [expert_gate, expert_up, expert_down]
    return pl.pallas_call(
        functools.partial(expert_kernel, parts),
        out_shape=[out] * parts,
        grid=(hidden // tile,),
        in_specs=[piece] * parts
        + [
            pl.BlockSpec((1, width, tile), lambda i: (0, 0, i)),
            pl.BlockSpec((1, width, tile), lambda i: (0, 0, i)),
            pl.BlockSpec((1, tile, width), lambda i: (0, i, 0)),
        ],
        out_specs=[piece] * parts,
        scratch_shapes=[
            pltpu.VMEM((parts * size, width), BF16),
            pltpu.VMEM((parts * size, width), F32),
        ],
        cost_estimate=cost(2 * parts * size * 3 * width * hidden, weights),
        name="expert_rows",
    )(*pieces, *weights)


def combine_kernel(parts, *refs):
    pieces, table = refs[:parts], refs[parts]
    full_ref, short_ref, high, low, rows = refs[parts + 1 :]
    size = pieces[0].shape[0]
    tokens = table.shape[2]
    slots = lax.broadcasted_iota(jnp.int32, (size, tokens), 0).astype(F32)
    for k in range(parts):
        at = slice(k * size, (k + 1) * size)
        weight = jnp.where(table[0, k : k + 1] == slots, table[1, k : k + 1], 0.0)
        top = weight.astype(BF16)
        high[at] = top
        low[at] = (weight - top.astype(F32)).astype(BF16)
        rows[at] = pieces[k][...]
    contract = (((0,), (0,)), ((), ()))
    total = lax.dot_general(high[...], rows[...], contract, preferred_element_type=F32)
    total += lax.dot_general(low[...], rows[...], contract, preferred_element_type=F32)
    full_ref[...] = total
    short_ref[...] = total.astype(BF16)


def combine(pieces, table):
    parts = len(pieces)
    size, width = pieces[0].shape
    tokens = table.shape[2]
    whole = pl.BlockSpec(memory_space=pltpu.VMEM)
    out_shape = [
        jax.ShapeDtypeStruct((tokens, width), F32),
        jax.ShapeDtypeStruct((tokens, width), BF16),
    ]
    return pl.pallas_call(
        functools.partial(combine_kernel, parts),
        out_shape=out_shape,
        in_specs=[whole] * (parts + 1),
        out_specs=[whole] * 2,
        scratch_shapes=[
            pltpu.VMEM((parts * size, tokens), BF16),
            pltpu.VMEM((parts * size, tokens), BF16),
            pltpu.VMEM((parts * size, width), BF16),
        ],
        cost_estimate=cost(4 * parts * size * tokens * width, out_shape),
        name="combine_rows",
    )(*pieces, table)


def swiglu_hidden(row_block, weight_gate, weight_up):
    gate_part = jnp.dot(row_block, weight_gate, preferred_element_type=F32)
    up_part = jnp.dot(row_block, weight_up, preferred_element_type=F32)
    return (jax.nn.silu(gate_part) * up_part).astype(BF16)


def gather_line(own, count):
    if count != 4:
        return [own] + [lax.ppermute(own, "z", flips(count, j)) for j in range(1, count)]
    sides, middle = flips(4, 1), [(1, 2), (2, 1)]
    near = lax.ppermute(own, "z", sides)
    across = lax.ppermute(own, "z", middle)
    across_far = lax.ppermute(near, "z", middle)
    side_far = lax.ppermute(across, "z", sides)
    side_end = lax.ppermute(across_far, "z", sides)
    return [own, near, across_far + side_far, across + side_end]


def exchange(pieces):
    count = len(pieces)
    moved = [lax.ppermute(pieces[k], PLANE, flips(count, k)) for k in range(1, count)]
    return [pieces[0]] + moved


def body(
    out_gate,
    in_gate,
    conv_values,
    conv_taps,
    mix_gain,
    out_proj,
    residual,
    ffn_gain,
    routes,
    route_weights,
    shared_gate,
    shared_up,
    shared_down,
    expert_gate,
    expert_up,
    expert_down,
):
    z_count, tp_count = lax.axis_size("z"), lax.axis_size("tp")
    plane_count = lax.axis_size("x") * tp_count
    experts_total = z_count * plane_count
    z_index, tp_index = lax.axis_index("z"), lax.axis_index("tp")
    plane_index = lax.axis_index("x") * tp_count + tp_index

    back = conv_taps.shape[0] - 1
    length = conv_values.shape[0]
    tail = in_gate[length - back :].astype(F32) * conv_values[length - back :].astype(F32)
    halo = from_behind(tail, 1)
    me = tp_index.reshape(1).astype(jnp.int32)
    blocks = filter_rows(me, out_gate, in_gate, conv_values, conv_taps, halo, tp_count)
    pieces = [blocks[0]] + [
        lax.ppermute(blocks[k], "tp", flips(tp_count, k)) for k in range(1, tp_count)
    ]

    row_count, top_count = routes.shape
    capacity = max(2, 4 * row_count * top_count // (3 * experts_total))
    gate_values = route_weights / jnp.sum(route_weights, axis=1, keepdims=True) * 2.5
    layers = jnp.arange(z_count, dtype=jnp.int32) ^ z_index
    places = jnp.arange(plane_count, dtype=jnp.int32) ^ plane_index
    experts = (layers[:, None] * plane_count + places[None, :]).reshape(-1)
    hits = routes.T[:, None, :] == experts[None, :, None]
    named = jnp.any(hits, axis=0)
    gates_of = jnp.sum(jnp.where(hits, gate_values.T[:, None, :], 0.0), axis=0)
    steps = jnp.arange(row_count, dtype=jnp.int32)
    earlier = (steps[:, None] < steps[None, :]).astype(BF16)
    rank = jnp.dot(named.astype(BF16), earlier, preferred_element_type=F32)
    rank = jnp.where(named, rank, -1.0)
    table = jnp.stack([rank, gates_of]).reshape(2, z_count, plane_count, row_count)
    tables = [table[:, 0]] + [
        lax.ppermute(table[:, j], "z", flips(z_count, j)) for j in range(1, z_count)
    ]

    stream, normed = mix_project(me, pieces, mix_gain, out_proj, residual, ffn_gain)

    slots = jnp.arange(capacity, dtype=jnp.int32).astype(F32)
    sources = gather_line(normed, z_count)
    arrived = []
    for j in range(z_count):
        pick = (tables[j][0][:, None, :] == slots[None, :, None]).astype(BF16)
        pick = pick.reshape(plane_count * capacity, row_count)
        outgoing = jnp.dot(pick, sources[j], preferred_element_type=F32).astype(BF16)
        arrived.append(
            exchange([outgoing[k * capacity : (k + 1) * capacity] for k in range(plane_count)])
        )

    shared_result = jnp.dot(
        swiglu_hidden(normed, shared_gate, shared_up), shared_down, preferred_element_type=F32
    )
    base = stream + shared_result

    results = [expert_rows(arrived[j], expert_gate, expert_up, expert_down) for j in range(z_count)]
    partial, short = [None] * z_count, [None] * z_count
    for j in reversed(range(z_count)):
        partial[j], short[j] = combine(exchange(results[j]), tables[j])

    if z_count == 4:
        outward, middle, sides = [(0, 1), (3, 2)], [(1, 2), (2, 1)], flips(4, 1)
        far = lax.ppermute(short[3], "z", outward).astype(F32)
        mid = lax.ppermute(short[2], "z", outward).astype(F32)
        far = lax.ppermute((far + partial[2]).astype(BF16), "z", middle).astype(F32)
        mid = lax.ppermute((mid + partial[3]).astype(BF16), "z", middle).astype(F32)
        last = lax.ppermute((far + partial[1]).astype(BF16), "z", sides).astype(F32)
        routed = partial[0] + mid + last
    else:
        routed = partial[0]
        for j in range(1, z_count):
            routed = routed + lax.ppermute(short[j], "z", flips(z_count, j))
    return (base + routed).astype(BF16)


def solution(mesh):
    sp_count, tp_count = mesh.shape["sp"], mesh.shape["tp"]
    z_count = 1 << -(-(sp_count.bit_length() - 1) // 2)
    split = Mesh(
        mesh.devices.reshape(z_count, sp_count // z_count, tp_count), ("z", "x", "tp")
    )
    every = ("z", "x", "tp")
    in_specs = (
        P(SEQ, "tp"),
        P(SEQ, "tp"),
        P(SEQ, "tp"),
        P(None, "tp"),
        P(),
        P(),
        P(every, None),
        P(),
        P(every, None),
        P(every, None),
        P(),
        P(),
        P(),
        P(every, None, None),
        P(every, None, None),
        P(every, None, None),
    )
    return jax.shard_map(
        body, mesh=split, in_specs=in_specs, out_specs=P(every, None), check_vma=False
    )
```

```python
import functools

import jax
import jax.numpy as jnp
from jax import lax
from jax.experimental import pallas as pl
from jax.experimental.pallas import tpu as pltpu
from jax.sharding import Mesh, PartitionSpec as P


SEQ, TP, CHIPS, PLANE = ("z", "x"), ("y", "c"), ("x", "y"), ("x", "y", "c")
BF16, F32 = jnp.bfloat16, jnp.float32


def flips(count, distance):
    return [(i, i ^ distance) for i in range(count)]


def from_behind(block, distance):
    count = lax.axis_size(SEQ)
    route = [(i - distance, i) for i in range(distance, count)]
    return lax.ppermute(block, SEQ, route)


def grant(mib):
    return pltpu.CompilerParams(vmem_limit_bytes=mib << 20)


def cost(flops, arrays):
    size = sum(a.size * a.dtype.itemsize for a in arrays)
    return pl.CostEstimate(flops=flops, bytes_accessed=size, transcendentals=0)


def filter_kernel(parts, taps_count, me_ref, gate_ref, in_ref, val_ref, taps_ref, halo_ref, *rest):
    outs, scratch = rest[:parts], rest[parts]
    length = val_ref.shape[0]
    rows = length // parts
    back = taps_count - 1
    scratch[0:8] = jnp.zeros((8, scratch.shape[1]), F32)
    scratch[8 - back : 8] = halo_ref[...]
    scratch[8:] = in_ref[...].astype(F32) * val_ref[...].astype(F32)
    me = me_ref[0]
    for k in range(parts):
        start = pl.multiple_of((me ^ k) * rows, 16)
        window = scratch[pl.ds(start, rows + 8)]
        total = taps_ref[0:1] * window[8 - back : 8 - back + rows]
        for offset in range(1, taps_count):
            first = 8 - back + offset
            total = total + taps_ref[offset : offset + 1] * window[first : first + rows]
        outs[k][...] = (gate_ref[pl.ds(start, rows)].astype(F32) * total).astype(BF16)


def filter_rows(me, out_gate, in_gate, conv_values, conv_taps, halo, parts):
    length, channels = conv_values.shape
    out = jax.ShapeDtypeStruct((length // parts, channels), BF16)
    whole = pl.BlockSpec(memory_space=pltpu.VMEM)
    return pl.pallas_call(
        functools.partial(filter_kernel, parts, conv_taps.shape[0]),
        out_shape=[out] * parts,
        in_specs=[pl.BlockSpec(memory_space=pltpu.SMEM)] + [whole] * 5,
        out_specs=[whole] * parts,
        scratch_shapes=[pltpu.VMEM((length + 8, channels), F32)],
        cost_estimate=cost(8 * out_gate.size, [out_gate, in_gate, conv_values]),
        compiler_params=grant(8),
        name="filter_rows",
    )(me, out_gate, in_gate, conv_values, conv_taps, halo)


def mix_kernel(parts, me_ref, *refs):
    pieces = refs[:parts]
    mix_gain, out_proj, residual, ffn_gain, stream_ref, normed_ref, acc, squares = refs[parts:]
    step = pl.program_id(0)

    @pl.when(step == 0)
    def _():
        acc[...] = jnp.zeros_like(acc)
        squares[...] = jnp.zeros_like(squares)

    for k in range(parts):

        @pl.when(step == k)
        def _(k=k):
            values = pieces[k][...].astype(F32)
            squares[...] += jnp.sum(values * values, axis=1, keepdims=True)
            scaled = (values * mix_gain[...].reshape(1, -1)).astype(BF16)
            acc[...] += jnp.dot(scaled, out_proj[...], preferred_element_type=F32)

    @pl.when(step == parts - 1)
    def _():
        channels = parts * pieces[0].shape[1]
        inverse = lax.rsqrt(squares[...] / channels + 1e-06)
        stream = residual[...].astype(F32) + acc[...] * inverse
        stream_ref[...] = stream
        mean = jnp.mean(stream * stream, axis=1, keepdims=True)
        normed_ref[...] = (stream * lax.rsqrt(mean + 1e-06) * ffn_gain[...]).astype(BF16)


def mix_project(me, pieces, mix_gain, out_proj, residual, ffn_gain):
    parts = len(pieces)
    rows, channels = pieces[0].shape
    width = out_proj.shape[1]
    fixed = lambda shape: pl.BlockSpec(shape, lambda i, me_ref: (0,) * len(shape))
    if channels % 128:
        gain = mix_gain.reshape(parts, 1, channels)
        gain_spec = pl.BlockSpec((1, 1, channels), lambda i, me_ref: (me_ref[0] ^ i, 0, 0))
    else:
        gain = mix_gain[None]
        gain_spec = pl.BlockSpec((1, channels), lambda i, me_ref: (0, me_ref[0] ^ i))
    out_shape = [
        jax.ShapeDtypeStruct((rows, width), F32),
        jax.ShapeDtypeStruct((rows, width), BF16),
    ]
    grid_spec = pltpu.PrefetchScalarGridSpec(
        num_scalar_prefetch=1,
        grid=(parts,),
        in_specs=[fixed((rows, channels))] * parts
        + [
            gain_spec,
            pl.BlockSpec((channels, width), lambda i, me_ref: (me_ref[0] ^ i, 0)),
            fixed((rows, width)),
            fixed((1, width)),
        ],
        out_specs=[fixed((rows, width))] * 2,
        scratch_shapes=[pltpu.VMEM((rows, width), F32), pltpu.VMEM((rows, 1), F32)],
    )
    return pl.pallas_call(
        functools.partial(mix_kernel, parts),
        out_shape=out_shape,
        grid_spec=grid_spec,
        cost_estimate=cost(2 * rows * out_proj.size, [out_proj, residual] + out_shape),
        compiler_params=grant(14),
        name="mix_project",
    )(me, *pieces, gain, out_proj, residual, ffn_gain[None])


def send_kernel(chips, own_ref, pair_ref, table_ref, *outs):
    size = outs[0].shape[0] // 2
    tokens = own_ref.shape[0]
    slots = lax.broadcasted_iota(jnp.int32, (size, tokens), 0).astype(F32)
    for side, (ref, base) in enumerate(((own_ref, 0), (pair_ref, 4 * chips))):
        pick = jnp.concatenate(
            [
                (table_ref[base + k : base + k + 1] == slots).astype(F32).astype(BF16)
                for k in range(chips)
            ]
        )
        rows = jnp.dot(pick, ref[...], preferred_element_type=F32).astype(BF16)
        for k in range(chips):
            outs[k][side * size : (side + 1) * size] = rows[k * size : (k + 1) * size]


def outgoing_rows(own, pair, table, chips, capacity):
    tokens, width = own.shape
    whole = pl.BlockSpec(memory_space=pltpu.VMEM)
    out_shape = [jax.ShapeDtypeStruct((2 * capacity, width), BF16)] * chips
    return pl.pallas_call(
        functools.partial(send_kernel, chips),
        out_shape=out_shape,
        in_specs=[whole] * 3,
        out_specs=[whole] * chips,
        cost_estimate=cost(4 * chips * capacity * tokens * width, [own, pair] + out_shape),
        compiler_params=grant(6),
        name="outgoing_rows",
    )(own, pair, table)


def swiglu_term(rows, gate_ref, up_ref, down_ref):
    gate_part = jnp.dot(rows, gate_ref, preferred_element_type=F32)
    up_part = jnp.dot(rows, up_ref, preferred_element_type=F32)
    hidden = (gate_part / (1.0 + jnp.exp(-gate_part)) * up_part).astype(BF16)
    return jnp.dot(hidden, down_ref, preferred_element_type=F32)


def expert_kernel(parts, count, *refs):
    pieces, outs = refs[:parts], refs[parts + 3 : parts + 3 + count]
    gate_ref, up_ref, down_ref = refs[parts : parts + 3]
    rows, acc = refs[parts + 3 + count :]
    size, out_size = pieces[0].shape[0], outs[0].shape[0]
    step = pl.program_id(0)

    @pl.when(step == 0)
    def _():
        for k in range(parts):
            rows[k * size : (k + 1) * size] = pieces[k][...]

    term = swiglu_term(rows[...], gate_ref[0], up_ref[0], down_ref[0])

    @pl.when(step == 0)
    def _():
        acc[...] = term

    @pl.when((step > 0) & (step < pl.num_programs(0) - 1))
    def _():
        acc[...] += term

    @pl.when(step == pl.num_programs(0) - 1)
    def _():
        total = acc[...] + term
        for k in range(count):
            outs[k][...] = total[k * out_size : (k + 1) * out_size].astype(BF16)


def expert_rows(pieces, count, expert_gate, expert_up, expert_down):
    parts = len(pieces)
    size, width = pieces[0].shape
    out_size = parts * size // count
    hidden = expert_gate.shape[2]
    tile = hidden // 2
    out = jax.ShapeDtypeStruct((out_size, width), BF16)
    weights = [expert_gate, expert_up, expert_down]
    return pl.pallas_call(
        functools.partial(expert_kernel, parts, count),
        out_shape=[out] * count,
        grid=(2,),
        in_specs=[pl.BlockSpec((size, width), lambda i: (0, 0))] * parts
        + [
            pl.BlockSpec((1, width, tile), lambda i: (0, 0, i)),
            pl.BlockSpec((1, width, tile), lambda i: (0, 0, i)),
            pl.BlockSpec((1, tile, width), lambda i: (0, i, 0)),
        ],
        out_specs=[pl.BlockSpec((out_size, width), lambda i: (0, 0))] * count,
        scratch_shapes=[
            pltpu.VMEM((parts * size, width), BF16),
            pltpu.VMEM((parts * size, width), F32),
        ],
        cost_estimate=cost(2 * parts * size * 3 * width * hidden, weights),
        compiler_params=grant(20),
        name="expert_rows",
    )(*pieces, *weights)


def shared_kernel(rows_ref, stream_ref, gate_ref, up_ref, down_ref, out_ref):
    term = swiglu_term(rows_ref[...], gate_ref[...], up_ref[...], down_ref[...])

    @pl.when(pl.program_id(0) == 0)
    def _():
        out_ref[...] = stream_ref[...] + term

    @pl.when(pl.program_id(0) > 0)
    def _():
        out_ref[...] += term


def shared_rows(normed, stream, gate, up, down):
    rows, width = normed.shape
    hidden = gate.shape[1]
    tile = hidden // 2
    fixed = pl.BlockSpec((rows, width), lambda i: (0, 0))
    return pl.pallas_call(
        shared_kernel,
        out_shape=jax.ShapeDtypeStruct((rows, width), F32),
        grid=(2,),
        in_specs=[
            fixed,
            fixed,
            pl.BlockSpec((width, tile), lambda i: (0, i)),
            pl.BlockSpec((width, tile), lambda i: (0, i)),
            pl.BlockSpec((tile, width), lambda i: (i, 0)),
        ],
        out_specs=fixed,
        cost_estimate=cost(6 * rows * width * hidden, [gate, up, down]),
        compiler_params=grant(12),
        name="shared_rows",
    )(normed, stream, gate, up, down)


def combine_kernel(parts, chips, *refs):
    pieces, table = refs[:parts], refs[parts]
    full_ref, short_ref, high, low, rows = refs[parts + 1 :]
    size = pieces[0].shape[0]
    tokens = table.shape[1]
    slots = lax.broadcasted_iota(jnp.int32, (size, tokens), 0).astype(F32)
    for k in range(parts):
        at = slice(k * size, (k + 1) * size)
        row = (k % 2) * chips + k // 2
        named = table[row : row + 1] == slots
        weight = jnp.where(named, table[2 * chips + row : 2 * chips + row + 1], 0.0)
        top = weight.astype(BF16)
        high[at] = top
        low[at] = (weight - top.astype(F32)).astype(BF16)
        rows[at] = pieces[k][...]
    contract = (((0,), (0,)), ((), ()))
    total = lax.dot_general(high[...], rows[...], contract, preferred_element_type=F32)
    total += lax.dot_general(low[...], rows[...], contract, preferred_element_type=F32)
    full_ref[...] = total
    short_ref[...] = total.astype(BF16)


def combine(pieces, table):
    parts = len(pieces)
    size, width = pieces[0].shape
    tokens = table.shape[1]
    whole = pl.BlockSpec(memory_space=pltpu.VMEM)
    out_shape = [
        jax.ShapeDtypeStruct((tokens, width), F32),
        jax.ShapeDtypeStruct((tokens, width), BF16),
    ]
    return pl.pallas_call(
        functools.partial(combine_kernel, parts, parts // 2),
        out_shape=out_shape,
        in_specs=[whole] * (parts + 1),
        out_specs=[whole] * 2,
        scratch_shapes=[
            pltpu.VMEM((parts * size, tokens), BF16),
            pltpu.VMEM((parts * size, tokens), BF16),
            pltpu.VMEM((parts * size, width), BF16),
        ],
        cost_estimate=cost(4 * parts * size * tokens * width, out_shape),
        compiler_params=grant(8),
        name="combine_rows",
    )(*pieces, table)


def gather_line(own, count):
    if count != 4:
        return [own] + [lax.ppermute(own, "z", flips(count, j)) for j in range(1, count)]
    sides, middle = flips(4, 1), [(1, 2), (2, 1)]
    near = lax.ppermute(own, "z", sides)
    across = lax.ppermute(own, "z", middle)
    across_far = lax.ppermute(near, "z", middle)
    side_far = lax.ppermute(across, "z", sides)
    side_end = lax.ppermute(across_far, "z", sides)
    return [own, near, across_far + side_far, across + side_end]


def exchange(pieces, axes):
    count = len(pieces)
    moved = [lax.ppermute(pieces[k], axes, flips(count, k)) for k in range(1, count)]
    return [pieces[0]] + moved


def layer(
    out_gate,
    in_gate,
    conv_values,
    conv_taps,
    mix_gain,
    out_proj,
    residual,
    ffn_gain,
    routes,
    route_weights,
    shared_gate,
    shared_up,
    shared_down,
    expert_gate,
    expert_up,
    expert_down,
):
    z_count, tp_count = lax.axis_size("z"), lax.axis_size(TP)
    chips = lax.axis_size(CHIPS)
    z_index, tp_index = lax.axis_index("z"), lax.axis_index(TP)
    chip_index, core_index = lax.axis_index(CHIPS), lax.axis_index("c")

    back = conv_taps.shape[0] - 1
    length = conv_values.shape[0]
    tail = in_gate[length - back :].astype(F32) * conv_values[length - back :].astype(F32)
    halo = from_behind(tail, 1)
    me = tp_index.reshape(1).astype(jnp.int32)
    blocks = filter_rows(me, out_gate, in_gate, conv_values, conv_taps, halo, tp_count)
    pieces = exchange(blocks, TP)

    row_count, top_count = routes.shape
    capacity = max(2, 4 * row_count * top_count // (6 * z_count * chips))
    gate_values = route_weights / jnp.sum(route_weights, axis=1, keepdims=True) * 2.5
    layers = jnp.arange(z_count, dtype=jnp.int32) ^ z_index
    cores = jnp.arange(2, dtype=jnp.int32) ^ core_index
    places = jnp.arange(chips, dtype=jnp.int32) ^ chip_index
    experts = (layers[:, None, None] * chips + places) * 2 + cores[:, None]
    hits = routes.T[:, None, :] == experts.reshape(-1)[None, :, None]
    named = jnp.any(hits, axis=0)
    gates_of = jnp.sum(jnp.where(hits, gate_values.T[:, None, :], 0.0), axis=0)
    steps = jnp.arange(row_count, dtype=jnp.int32)
    earlier = (steps[:, None] < steps[None, :]).astype(BF16)
    rank = jnp.dot(named.astype(BF16), earlier, preferred_element_type=F32)
    rank = jnp.where(named, rank, -1.0).reshape(z_count, 2 * chips, row_count)
    gates_of = gates_of.reshape(z_count, 2 * chips, row_count)
    pair_rank = lax.ppermute(rank[:, chips:], "c", flips(2, 1))
    table = jnp.concatenate([rank, gates_of, pair_rank], axis=1)
    tables = [table[0]] + [
        lax.ppermute(table[j], "z", flips(z_count, j))
        for j in range(1, z_count)
    ]

    stream, normed = mix_project(me, pieces, mix_gain, out_proj, residual, ffn_gain)

    sources = gather_line(normed, z_count)
    results = []
    for j in range(z_count):
        pair = lax.ppermute(sources[j], "c", flips(2, 1))
        outgoing = outgoing_rows(sources[j], pair, tables[j], chips, capacity)
        arrived = exchange(outgoing, CHIPS)
        weights = (expert_gate, expert_up, expert_down)
        results.append(expert_rows(arrived, 2 * chips, *weights))

    base = shared_rows(normed, stream, shared_gate, shared_up, shared_down)

    partial, short = [None] * z_count, [None] * z_count
    for j in reversed(range(z_count)):
        returned = exchange(results[j], PLANE)
        partial[j], short[j] = combine(returned, tables[j])

    if z_count == 4:
        outward, middle, sides = [(0, 1), (3, 2)], [(1, 2), (2, 1)], flips(4, 1)

        def hop(block, route):
            return lax.ppermute(block.astype(BF16), "z", route).astype(F32)

        far = hop(short[3], outward)
        mid = hop(short[2], outward)
        far = hop(far + partial[2], middle)
        mid = hop(mid + partial[3], middle)
        last = hop(far + partial[1], sides)
        routed = partial[0] + mid + last
    else:
        routed = partial[0]
        for j in range(1, z_count):
            routed = routed + lax.ppermute(short[j], "z", flips(z_count, j))
    return (base + routed).astype(BF16)


def solution(mesh):
    sp_count, tp_count = mesh.shape["sp"], mesh.shape["tp"]
    z_count = 1 << -(-(sp_count.bit_length() - 1) // 2)
    every = SEQ + TP
    split = Mesh(
        mesh.devices.reshape(z_count, sp_count // z_count, tp_count // 2, 2), every
    )
    in_specs = (
        P(SEQ, TP),
        P(SEQ, TP),
        P(SEQ, TP),
        P(None, TP),
        P(),
        P(),
        P(every, None),
        P(),
        P(every, None),
        P(every, None),
        P(),
        P(),
        P(),
        P(every, None, None),
        P(every, None, None),
        P(every, None, None),
    )
    return jax.shard_map(
        layer, mesh=split, in_specs=in_specs, out_specs=P(every, None), check_vma=False
    )
```

```python
import functools

import jax
import jax.numpy as jnp
from jax import lax
from jax.experimental import pallas as pl
from jax.experimental.pallas import tpu as pltpu
from jax.sharding import Mesh, PartitionSpec as P


SEQ, TP, CHIPS, PLANE = ("z", "x"), ("y", "c"), ("x", "y"), ("x", "y", "c")
MIDDLE = [(1, 2), (2, 1)]
BF16, F32 = jnp.bfloat16, jnp.float32


def flips(count, distance):
    return [(i, i ^ distance) for i in range(count)]


def from_behind(block, distance):
    count = lax.axis_size(SEQ)
    route = [((i - distance) % count, i) for i in range(count)]
    return lax.ppermute(block, SEQ, route)


def grant(mib):
    return pltpu.CompilerParams(vmem_limit_bytes=mib << 20)


def cost(flops, arrays):
    size = sum(a.size * a.dtype.itemsize for a in arrays)
    return pl.CostEstimate(flops=flops, bytes_accessed=size, transcendentals=0)


def filter_kernel(parts, back, me_ref, gate_ref, in_ref, val_ref, taps_ref, *rest):
    outs, head_ref, scratch = rest[:parts], rest[parts], rest[parts + 1]
    length = val_ref.shape[0]
    rows = length // parts
    scratch[0:8] = jnp.zeros((8, scratch.shape[1]), F32)
    scratch[8:] = in_ref[...].astype(F32) * val_ref[...].astype(F32)
    me = me_ref[0]
    for k in range(parts):
        start = pl.multiple_of((me ^ k) * rows, 16)
        window = scratch[pl.ds(start, rows + 8)]
        total = taps_ref[0:1] * window[8 - back : 8 - back + rows]
        for offset in range(1, back + 1):
            first = 8 - back + offset
            total = total + taps_ref[offset : offset + 1] * window[first : first + rows]
        outs[k][...] = (gate_ref[pl.ds(start, rows)].astype(F32) * total).astype(BF16)
    window = scratch[0:24]
    total = taps_ref[0:1] * window[8 - back : 24 - back]
    for offset in range(1, back + 1):
        first = 8 - back + offset
        total = total + taps_ref[offset : offset + 1] * window[first : first + 16]
    head_ref[0:16] = total
    head_ref[16:32] = gate_ref[0:16].astype(F32)


def filter_rows(me, out_gate, in_gate, conv_values, conv_taps, parts):
    length, channels = conv_values.shape
    out = jax.ShapeDtypeStruct((length // parts, channels), BF16)
    whole = pl.BlockSpec(memory_space=pltpu.VMEM)
    *blocks, head = pl.pallas_call(
        functools.partial(filter_kernel, parts, conv_taps.shape[0] - 1),
        out_shape=[pltpu.VMEM(out.shape, BF16)] * parts + [pltpu.VMEM((32, channels), F32)],
        in_specs=[pl.BlockSpec(memory_space=pltpu.SMEM)] + [whole] * 4,
        out_specs=[whole] * (parts + 1),
        scratch_shapes=[pltpu.VMEM((length + 8, channels), F32)],
        cost_estimate=cost(1 << 20, [out_gate, in_gate, conv_values]),
        name="filter_rows",
    )(me, out_gate, in_gate, conv_values, conv_taps)
    return blocks, head


def mend_kernel(parts, back, me_ref, head_ref, taps_ref, halo_ref, *refs):
    outs = refs[parts:]
    channels = head_ref.shape[1]
    row = lax.broadcasted_iota(jnp.int32, (16, channels), 0)
    total = head_ref[0:16]
    for offset in range(back):
        for at_row in range(back - offset):
            term = taps_ref[offset : offset + 1] * halo_ref[at_row + offset : at_row + offset + 1]
            total = total + jnp.where((row == at_row) & (me_ref[1] > 0), term, 0.0)
    fresh = (head_ref[16:32] * total).astype(BF16)
    for k in range(parts):

        @pl.when(me_ref[0] == k)
        def _(k=k):
            outs[k][0:16] = fresh


def mend_rows(me, blocks, head, conv_taps, halo):
    parts = len(blocks)
    whole = pl.BlockSpec(memory_space=pltpu.VMEM)
    return pl.pallas_call(
        functools.partial(mend_kernel, parts, conv_taps.shape[0] - 1),
        out_shape=[pltpu.VMEM(blocks[0].shape, BF16)] * parts,
        in_specs=[pl.BlockSpec(memory_space=pltpu.SMEM)] + [whole] * (3 + parts),
        out_specs=[whole] * parts,
        input_output_aliases={4 + k: k for k in range(parts)},
        cost_estimate=cost(1 << 20, blocks),
        compiler_params=grant(8),
        name="mend_rows",
    )(me, head, conv_taps, halo, *blocks)


def fetch_kernel(from_ref, to_ref, sem):
    copy = pltpu.make_async_copy(from_ref, to_ref, sem)
    copy.start()
    copy.wait()


def fetch(array):
    return pl.pallas_call(
        fetch_kernel,
        out_shape=pltpu.VMEM(array.shape, array.dtype),
        in_specs=[pl.BlockSpec(memory_space=pltpu.HBM)],
        out_specs=pl.BlockSpec(memory_space=pltpu.VMEM),
        scratch_shapes=[pltpu.SemaphoreType.DMA],
        cost_estimate=cost(1 << 20, [array]),
        compiler_params=grant(1),
        name="fetch_rows",
    )(array)


def mix_kernel(parts, me_ref, *refs):
    pieces = refs[:parts]
    mix_gain, out_proj, residual, ffn_gain, stream_ref, normed_ref, acc, squares = refs[parts:]
    step = pl.program_id(0)

    @pl.when(step == 0)
    def _():
        acc[...] = jnp.zeros_like(acc)
        squares[...] = jnp.zeros_like(squares)

    for k in range(parts):

        @pl.when(step == k)
        def _(k=k):
            values = pieces[k][...].astype(F32)
            squares[...] += jnp.sum(values * values, axis=1, keepdims=True)
            scaled = (values * mix_gain[...].reshape(1, -1)).astype(BF16)
            acc[...] += jnp.dot(scaled, out_proj[...], preferred_element_type=F32)

    @pl.when(step == parts - 1)
    def _():
        channels = parts * pieces[0].shape[1]
        inverse = lax.rsqrt(squares[...] / channels + 1e-06)
        stream = residual[...].astype(F32) + acc[...] * inverse
        stream_ref[...] = stream
        mean = jnp.mean(stream * stream, axis=1, keepdims=True)
        normed_ref[...] = (stream * lax.rsqrt(mean + 1e-06) * ffn_gain[...]).astype(BF16)


def mix_project(me, pieces, mix_gain, out_proj, residual, ffn_gain):
    parts = len(pieces)
    rows, channels = pieces[0].shape
    width = out_proj.shape[1]
    fixed = lambda shape: pl.BlockSpec(shape, lambda i, me_ref: (0,) * len(shape))
    if channels % 128:
        gain = mix_gain.reshape(parts, 1, channels)
        gain_spec = pl.BlockSpec((1, 1, channels), lambda i, me_ref: (me_ref[0] ^ i, 0, 0))
    else:
        gain = mix_gain[None]
        gain_spec = pl.BlockSpec((1, channels), lambda i, me_ref: (0, me_ref[0] ^ i))
    out_shape = [
        jax.ShapeDtypeStruct((rows, width), F32),
        jax.ShapeDtypeStruct((rows, width), BF16),
    ]
    grid_spec = pltpu.PrefetchScalarGridSpec(
        num_scalar_prefetch=1,
        grid=(parts,),
        in_specs=[fixed((rows, channels))] * parts
        + [
            gain_spec,
            pl.BlockSpec((channels, width), lambda i, me_ref: (me_ref[0] ^ i, 0)),
            fixed((rows, width)),
            fixed((1, width)),
        ],
        out_specs=[fixed((rows, width))] * 2,
        scratch_shapes=[pltpu.VMEM((rows, width), F32), pltpu.VMEM((rows, 1), F32)],
    )
    return pl.pallas_call(
        functools.partial(mix_kernel, parts),
        out_shape=out_shape,
        grid_spec=grid_spec,
        cost_estimate=cost(2 * rows * out_proj.size, [out_proj, residual] + out_shape),
        compiler_params=grant(14),
        name="mix_project",
    )(me, *pieces, gain, out_proj, residual, ffn_gain[None])


def send_kernel(chips, own_ref, pair_ref, table_ref, *outs):
    size = outs[0].shape[0] // 2
    tokens = own_ref.shape[0]
    slots = lax.broadcasted_iota(jnp.int32, (size, tokens), 0).astype(F32)
    for side, (ref, base) in enumerate(((own_ref, 0), (pair_ref, 4 * chips))):
        pick = jnp.concatenate(
            [
                (table_ref[base + k : base + k + 1] == slots).astype(F32).astype(BF16)
                for k in range(chips)
            ]
        )
        rows = jnp.dot(pick, ref[...], preferred_element_type=F32).astype(BF16)
        for k in range(chips):
            outs[k][side * size : (side + 1) * size] = rows[k * size : (k + 1) * size]


def outgoing_rows(own, pair, table, chips, capacity):
    tokens, width = own.shape
    whole = pl.BlockSpec(memory_space=pltpu.VMEM)
    out_shape = [jax.ShapeDtypeStruct((2 * capacity, width), BF16)] * chips
    return pl.pallas_call(
        functools.partial(send_kernel, chips),
        out_shape=out_shape,
        in_specs=[whole] * 3,
        out_specs=[whole] * chips,
        cost_estimate=cost(4 * chips * capacity * tokens * width, [own, pair] + out_shape),
        compiler_params=grant(6),
        name="outgoing_rows",
    )(own, pair, table)


def swiglu_term(rows, gate_ref, up_ref, down_ref):
    gate_part = jnp.dot(rows, gate_ref, preferred_element_type=F32)
    up_part = jnp.dot(rows, up_ref, preferred_element_type=F32)
    hidden = (gate_part / (1.0 + jnp.exp(-gate_part)) * up_part).astype(BF16)
    return jnp.dot(hidden, down_ref, preferred_element_type=F32)


def expert_kernel(parts, count, *refs):
    pieces, outs = refs[:parts], refs[parts + 3 : parts + 3 + count]
    gate_ref, up_ref, down_ref = refs[parts : parts + 3]
    rows, acc = refs[parts + 3 + count :]
    size, out_size = pieces[0].shape[0], outs[0].shape[0]
    step = pl.program_id(0)

    @pl.when(step == 0)
    def _():
        for k in range(parts):
            rows[k * size : (k + 1) * size] = pieces[k][...]

    term = swiglu_term(rows[...], gate_ref[0], up_ref[0], down_ref[0])

    @pl.when(step == 0)
    def _():
        acc[...] = term

    @pl.when((step > 0) & (step < pl.num_programs(0) - 1))
    def _():
        acc[...] += term

    @pl.when(step == pl.num_programs(0) - 1)
    def _():
        total = acc[...] + term
        for k in range(count):
            outs[k][...] = total[k * out_size : (k + 1) * out_size].astype(BF16)


def expert_rows(pieces, count, expert_gate, expert_up, expert_down):
    parts = len(pieces)
    size, width = pieces[0].shape
    out_size = parts * size // count
    hidden = expert_gate.shape[2]
    tile = hidden // 2
    out = jax.ShapeDtypeStruct((out_size, width), BF16)
    weights = [expert_gate, expert_up, expert_down]
    return pl.pallas_call(
        functools.partial(expert_kernel, parts, count),
        out_shape=[out] * count,
        grid=(2,),
        in_specs=[pl.BlockSpec((size, width), lambda i: (0, 0))] * parts
        + [
            pl.BlockSpec((1, width, tile), lambda i: (0, 0, i)),
            pl.BlockSpec((1, width, tile), lambda i: (0, 0, i)),
            pl.BlockSpec((1, tile, width), lambda i: (0, i, 0)),
        ],
        out_specs=[pl.BlockSpec((out_size, width), lambda i: (0, 0))] * count,
        scratch_shapes=[
            pltpu.VMEM((parts * size, width), BF16),
            pltpu.VMEM((parts * size, width), F32),
        ],
        cost_estimate=cost(2 * parts * size * 3 * width * hidden, weights),
        compiler_params=grant(20),
        name="expert_rows",
    )(*pieces, *weights)


def shared_kernel(rows_ref, stream_ref, gate_ref, up_ref, down_ref, out_ref):
    term = swiglu_term(rows_ref[...], gate_ref[...], up_ref[...], down_ref[...])

    @pl.when(pl.program_id(0) == 0)
    def _():
        out_ref[...] = stream_ref[...] + term

    @pl.when(pl.program_id(0) > 0)
    def _():
        out_ref[...] += term


def shared_rows(normed, stream, gate, up, down):
    rows, width = normed.shape
    hidden = gate.shape[1]
    tile = hidden // 2
    fixed = pl.BlockSpec((rows, width), lambda i: (0, 0))
    return pl.pallas_call(
        shared_kernel,
        out_shape=jax.ShapeDtypeStruct((rows, width), F32),
        grid=(2,),
        in_specs=[
            fixed,
            fixed,
            pl.BlockSpec((width, tile), lambda i: (0, i)),
            pl.BlockSpec((width, tile), lambda i: (0, i)),
            pl.BlockSpec((tile, width), lambda i: (i, 0)),
        ],
        out_specs=fixed,
        cost_estimate=cost(6 * rows * width * hidden, [gate, up, down]),
        compiler_params=grant(12),
        name="shared_rows",
    )(normed, stream, gate, up, down)


def combine_kernel(parts, chips, *refs):
    pieces, table = refs[:parts], refs[parts]
    full_ref, short_ref, high, low, rows = refs[parts + 1 :]
    size = pieces[0].shape[0]
    tokens = table.shape[1]
    slots = lax.broadcasted_iota(jnp.int32, (size, tokens), 0).astype(F32)
    for k in range(parts):
        at = slice(k * size, (k + 1) * size)
        row = (k % 2) * chips + k // 2
        named = table[row : row + 1] == slots
        weight = jnp.where(named, table[2 * chips + row : 2 * chips + row + 1], 0.0)
        top = weight.astype(BF16)
        high[at] = top
        low[at] = (weight - top.astype(F32)).astype(BF16)
        rows[at] = pieces[k][...]
    contract = (((0,), (0,)), ((), ()))
    total = lax.dot_general(high[...], rows[...], contract, preferred_element_type=F32)
    total += lax.dot_general(low[...], rows[...], contract, preferred_element_type=F32)
    full_ref[...] = total
    short_ref[...] = total.astype(BF16)


def combine(pieces, table):
    parts = len(pieces)
    size, width = pieces[0].shape
    tokens = table.shape[1]
    whole = pl.BlockSpec(memory_space=pltpu.VMEM)
    out_shape = [
        jax.ShapeDtypeStruct((tokens, width), F32),
        jax.ShapeDtypeStruct((tokens, width), BF16),
    ]
    return pl.pallas_call(
        functools.partial(combine_kernel, parts, parts // 2),
        out_shape=out_shape,
        in_specs=[whole] * (parts + 1),
        out_specs=[whole] * 2,
        scratch_shapes=[
            pltpu.VMEM((parts * size, tokens), BF16),
            pltpu.VMEM((parts * size, tokens), BF16),
            pltpu.VMEM((parts * size, width), BF16),
        ],
        cost_estimate=cost(4 * parts * size * tokens * width, out_shape),
        compiler_params=grant(8),
        name="combine_rows",
    )(*pieces, table)


def gather_line(own, count):
    if count != 4:
        return [own] + [lax.ppermute(own, "z", flips(count, j)) for j in range(1, count)]
    sides, middle = flips(4, 1), MIDDLE
    near = lax.ppermute(own, "z", sides)
    across = lax.ppermute(own, "z", middle)
    across_far = lax.ppermute(near, "z", middle)
    side_far = lax.ppermute(across, "z", sides)
    side_end = lax.ppermute(across_far, "z", sides)
    return [own, near, across_far + side_far, across + side_end]


def exchange(pieces, axes):
    count = len(pieces)
    moved = [lax.ppermute(pieces[k], axes, flips(count, k)) for k in range(1, count)]
    return [pieces[0]] + moved


def layer(
    out_gate,
    in_gate,
    conv_values,
    conv_taps,
    mix_gain,
    out_proj,
    residual,
    ffn_gain,
    routes,
    route_weights,
    shared_gate,
    shared_up,
    shared_down,
    expert_gate,
    expert_up,
    expert_down,
):
    z_count, tp_count = lax.axis_size("z"), lax.axis_size(TP)
    chips = lax.axis_size(CHIPS)
    z_index, tp_index = lax.axis_index("z"), lax.axis_index(TP)
    chip_index, core_index = lax.axis_index(CHIPS), lax.axis_index("c")

    back = conv_taps.shape[0] - 1
    length = conv_values.shape[0]
    tail = in_gate[length - back :].astype(F32) * conv_values[length - back :].astype(F32)
    halo = from_behind(tail, 1)
    me = jnp.stack([tp_index, lax.axis_index(SEQ)]).astype(jnp.int32)
    blocks, head = filter_rows(me, out_gate, in_gate, conv_values, conv_taps, tp_count)
    blocks = mend_rows(me, blocks, head, conv_taps, halo)
    pieces = exchange(blocks, TP)
    out_proj = fetch(out_proj)

    row_count, top_count = routes.shape
    capacity = max(2, 4 * row_count * top_count // (6 * z_count * chips))
    gate_values = route_weights / jnp.sum(route_weights, axis=1, keepdims=True) * 2.5
    layers = jnp.arange(z_count, dtype=jnp.int32) ^ z_index
    cores = jnp.arange(2, dtype=jnp.int32) ^ core_index
    places = jnp.arange(chips, dtype=jnp.int32) ^ chip_index
    experts = (layers[:, None, None] * chips + places) * 2 + cores[:, None]
    hits = routes.T[:, None, :] == experts.reshape(-1)[None, :, None]
    named = jnp.any(hits, axis=0)
    gates_of = jnp.sum(jnp.where(hits, gate_values.T[:, None, :], 0.0), axis=0)
    steps = jnp.arange(row_count, dtype=jnp.int32)
    earlier = (steps[:, None] < steps[None, :]).astype(BF16)
    rank = jnp.dot(named.astype(BF16), earlier, preferred_element_type=F32)
    rank = jnp.where(named, rank, -1.0).reshape(z_count, 2 * chips, row_count)
    gates_of = gates_of.reshape(z_count, 2 * chips, row_count)
    pair_rank = lax.ppermute(rank[:, chips:], "c", flips(2, 1))
    table = jnp.concatenate([rank, gates_of, pair_rank], axis=1)
    tables = [table[0]] + [
        lax.ppermute(table[j], "z", flips(z_count, j))
        for j in range(1, z_count)
    ]

    stream, normed = mix_project(me, pieces, mix_gain, out_proj, residual, ffn_gain)

    sources = gather_line(normed, z_count)
    results = []
    for j in range(z_count):
        pair = lax.ppermute(sources[j], "c", flips(2, 1))
        outgoing = outgoing_rows(sources[j], pair, tables[j], chips, capacity)
        arrived = exchange(outgoing, CHIPS)
        weights = (expert_gate, expert_up, expert_down)
        results.append(expert_rows(arrived, 2 * chips, *weights))

    base = shared_rows(normed, stream, shared_gate, shared_up, shared_down)

    partial, short = [None] * z_count, [None] * z_count
    for j in reversed(range(z_count)):
        returned = exchange(results[j], PLANE)
        partial[j], short[j] = combine(returned, tables[j])

    if z_count == 4:
        sides = flips(4, 1)

        def hop(block, route):
            return lax.ppermute(block.astype(BF16), "z", route).astype(F32)

        far = hop(short[3], sides)
        mid = hop(short[2], sides)
        far = hop(far + partial[2], MIDDLE)
        mid = hop(mid + partial[3], MIDDLE)
        last = hop(far + partial[1], sides)
        routed = partial[0] + mid + last
    else:
        routed = partial[0]
        for j in range(1, z_count):
            routed = routed + lax.ppermute(short[j], "z", flips(z_count, j))
    return (base + routed).astype(BF16)


def solution(mesh):
    sp_count, tp_count = mesh.shape["sp"], mesh.shape["tp"]
    z_count = 1 << -(-(sp_count.bit_length() - 1) // 2)
    every = SEQ + TP
    split = Mesh(
        mesh.devices.reshape(z_count, sp_count // z_count, tp_count // 2, 2), every
    )
    in_specs = (
        P(SEQ, TP),
        P(SEQ, TP),
        P(SEQ, TP),
        P(None, TP),
        P(),
        P(),
        P(every, None),
        P(),
        P(every, None),
        P(every, None),
        P(),
        P(),
        P(),
        P(every, None, None),
        P(every, None, None),
        P(every, None, None),
    )
    return jax.shard_map(
        layer, mesh=split, in_specs=in_specs, out_specs=P(every, None), check_vma=False
    )
```

```python
import functools

import jax
import jax.numpy as jnp
from jax import lax
from jax.experimental import pallas as pl
from jax.experimental.pallas import tpu as pltpu
from jax.sharding import Mesh, PartitionSpec as P


SEQ, TP, CHIPS, PLANE = ("z", "x"), ("y", "c"), ("x", "y"), ("x", "y", "c")
BF16, F32 = jnp.bfloat16, jnp.float32


def flips(count, distance):
    return [(i, i ^ distance) for i in range(count)]


def from_behind(block, distance):
    count = lax.axis_size(SEQ)
    route = [((i - distance) % count, i) for i in range(count)]
    return lax.ppermute(block, SEQ, route)


def grant(mib):
    return pltpu.CompilerParams(vmem_limit_bytes=mib << 20)


def cost(flops, arrays):
    size = sum(a.size * a.dtype.itemsize for a in arrays)
    return pl.CostEstimate(flops=flops, bytes_accessed=size, transcendentals=0)


def filter_kernel(parts, back, me_ref, gate_ref, in_ref, val_ref, taps_ref, *rest):
    outs, head_ref, scratch = rest[:parts], rest[parts], rest[parts + 1]
    length = val_ref.shape[0]
    rows = length // parts
    scratch[0:8] = jnp.zeros((8, scratch.shape[1]), F32)
    scratch[8:] = in_ref[...].astype(F32) * val_ref[...].astype(F32)
    me = me_ref[0]
    for k in range(parts):
        start = pl.multiple_of((me ^ k) * rows, 16)
        window = scratch[pl.ds(start, rows + 8)]
        total = taps_ref[0:1] * window[8 - back : 8 - back + rows]
        for offset in range(1, back + 1):
            first = 8 - back + offset
            total = total + taps_ref[offset : offset + 1] * window[first : first + rows]
        outs[k][...] = (gate_ref[pl.ds(start, rows)].astype(F32) * total).astype(BF16)
    window = scratch[0:24]
    total = taps_ref[0:1] * window[8 - back : 24 - back]
    for offset in range(1, back + 1):
        first = 8 - back + offset
        total = total + taps_ref[offset : offset + 1] * window[first : first + 16]
    head_ref[0:16] = total
    head_ref[16:32] = gate_ref[0:16].astype(F32)
    head_ref[32 : 33 + back] = taps_ref[...]


def filter_rows(me, out_gate, in_gate, conv_values, conv_taps, parts):
    length, channels = conv_values.shape
    out = jax.ShapeDtypeStruct((length // parts, channels), BF16)
    whole = pl.BlockSpec(memory_space=pltpu.VMEM)
    *blocks, head = pl.pallas_call(
        functools.partial(filter_kernel, parts, conv_taps.shape[0] - 1),
        out_shape=[pltpu.VMEM(out.shape, BF16)] * parts + [pltpu.VMEM((40, channels), F32)],
        in_specs=[pl.BlockSpec(memory_space=pltpu.SMEM)] + [whole] * 4,
        out_specs=[whole] * (parts + 1),
        scratch_shapes=[pltpu.VMEM((length + 8, channels), F32)],
        cost_estimate=cost(1 << 20, [out_gate, in_gate, conv_values]),
        name="filter_rows",
    )(me, out_gate, in_gate, conv_values, conv_taps)
    return blocks, head


def mend_kernel(parts, back, me_ref, seq_ref, head_ref, halo_ref, *refs):
    outs = refs[parts:]
    channels = head_ref.shape[1]
    row = lax.broadcasted_iota(jnp.int32, (16, channels), 0)
    total = head_ref[0:16]
    for offset in range(back):
        for at_row in range(back - offset):
            tap = head_ref[32 + offset : 33 + offset]
            term = tap * halo_ref[at_row + offset : at_row + offset + 1]
            total = total + jnp.where((row == at_row) & (seq_ref[0] > 0), term, 0.0)
    fresh = (head_ref[16:32] * total).astype(BF16)
    for k in range(parts):

        @pl.when(me_ref[0] == k)
        def _(k=k):
            outs[k][0:16] = fresh


def mend_rows(me, seq, blocks, head, back, halo):
    parts = len(blocks)
    whole = pl.BlockSpec(memory_space=pltpu.VMEM)
    return pl.pallas_call(
        functools.partial(mend_kernel, parts, back),
        out_shape=[pltpu.VMEM(blocks[0].shape, BF16)] * parts,
        in_specs=[pl.BlockSpec(memory_space=pltpu.SMEM)] * 2 + [whole] * (2 + parts),
        out_specs=[whole] * parts,
        input_output_aliases={4 + k: k for k in range(parts)},
        cost_estimate=cost(1 << 20, blocks),
        compiler_params=grant(8),
        name="mend_rows",
    )(me, seq, head, halo, *blocks)


def fetch_kernel(from_ref, to_ref, sem):
    copy = pltpu.make_async_copy(from_ref, to_ref, sem)
    copy.start()
    copy.wait()


def fetch(array):
    return pl.pallas_call(
        fetch_kernel,
        out_shape=pltpu.VMEM(array.shape, array.dtype),
        in_specs=[pl.BlockSpec(memory_space=pltpu.HBM)],
        out_specs=pl.BlockSpec(memory_space=pltpu.VMEM),
        scratch_shapes=[pltpu.SemaphoreType.DMA],
        cost_estimate=cost(1 << 20, [array]),
        compiler_params=grant(54),
        name="fetch_rows",
    )(array)


def mix_kernel(parts, me_ref, *refs):
    pieces = refs[:parts]
    mix_gain, out_proj, residual, ffn_gain, stream_ref, normed_ref, acc, squares = refs[parts:]
    step = pl.program_id(0)

    @pl.when(step == 0)
    def _():
        acc[...] = jnp.zeros_like(acc)
        squares[...] = jnp.zeros_like(squares)

    for k in range(parts):

        @pl.when(step == k)
        def _(k=k):
            values = pieces[k][...].astype(F32)
            squares[...] += jnp.sum(values * values, axis=1, keepdims=True)
            scaled = (values * mix_gain[...].reshape(1, -1)).astype(BF16)
            acc[...] += jnp.dot(scaled, out_proj[...], preferred_element_type=F32)

    @pl.when(step == parts - 1)
    def _():
        channels = parts * pieces[0].shape[1]
        inverse = lax.rsqrt(squares[...] / channels + 1e-06)
        stream = residual[...].astype(F32) + acc[...] * inverse
        stream_ref[...] = stream
        mean = jnp.mean(stream * stream, axis=1, keepdims=True)
        normed_ref[...] = (stream * lax.rsqrt(mean + 1e-06) * ffn_gain[...]).astype(BF16)


def mix_project(me, pieces, mix_gain, out_proj, residual, ffn_gain):
    parts = len(pieces)
    rows, channels = pieces[0].shape
    width = out_proj.shape[1]
    fixed = lambda shape: pl.BlockSpec(shape, lambda i, me_ref: (0,) * len(shape))
    if channels % 128:
        gain = mix_gain.reshape(parts, 1, channels)
        gain_spec = pl.BlockSpec((1, 1, channels), lambda i, me_ref: (me_ref[0] ^ i, 0, 0))
    else:
        gain = mix_gain[None]
        gain_spec = pl.BlockSpec((1, channels), lambda i, me_ref: (0, me_ref[0] ^ i))
    out_shape = [
        pltpu.HBM((rows, width), F32),
        jax.ShapeDtypeStruct((rows, width), BF16),
    ]
    grid_spec = pltpu.PrefetchScalarGridSpec(
        num_scalar_prefetch=1,
        grid=(parts,),
        in_specs=[fixed((rows, channels))] * parts
        + [
            gain_spec,
            pl.BlockSpec((channels, width), lambda i, me_ref: (me_ref[0] ^ i, 0)),
            fixed((rows, width)),
            fixed((1, width)),
        ],
        out_specs=[fixed((rows, width))] * 2,
        scratch_shapes=[pltpu.VMEM((rows, width), F32), pltpu.VMEM((rows, 1), F32)],
    )
    return pl.pallas_call(
        functools.partial(mix_kernel, parts),
        out_shape=out_shape,
        grid_spec=grid_spec,
        cost_estimate=cost(2 * rows * out_proj.size, [out_proj, residual]),
        compiler_params=grant(14),
        name="mix_project",
    )(me, *pieces, gain, out_proj, residual, ffn_gain[None])


def send_kernel(chips, base, own_ref, pair_ref, table_ref, *outs):
    size = outs[0].shape[0] // 2
    tokens = own_ref.shape[0]
    slots = lax.broadcasted_iota(jnp.int32, (size, tokens), 0).astype(F32)
    for side, (ref, first) in enumerate(((own_ref, 0), (pair_ref, base))):
        pick = jnp.concatenate(
            [
                (table_ref[first + k : first + k + 1] == slots).astype(F32).astype(BF16)
                for k in range(chips)
            ]
        )
        rows = jnp.dot(pick, ref[...], preferred_element_type=F32).astype(BF16)
        for k in range(chips):
            outs[k][side * size : (side + 1) * size] = rows[k * size : (k + 1) * size]


def outgoing_rows(own, pair, table, chips, capacity):
    tokens, width = own.shape
    whole = pl.BlockSpec(memory_space=pltpu.VMEM)
    out_shape = [jax.ShapeDtypeStruct((2 * capacity, width), BF16)] * chips
    return pl.pallas_call(
        functools.partial(send_kernel, chips, table.shape[0] - chips),
        out_shape=out_shape,
        in_specs=[whole] * 3,
        out_specs=[whole] * chips,
        cost_estimate=cost(4 * chips * capacity * tokens * width, [own, pair] + out_shape),
        compiler_params=grant(6),
        name="outgoing_rows",
    )(own, pair, table)


def swiglu_term(rows, gate_ref, up_ref, down_ref):
    gate_part = jnp.dot(rows, gate_ref, preferred_element_type=F32)
    up_part = jnp.dot(rows, up_ref, preferred_element_type=F32)
    hidden = (gate_part / (1.0 + jnp.exp(-gate_part)) * up_part).astype(BF16)
    return jnp.dot(hidden, down_ref, preferred_element_type=F32)


def expert_kernel(parts, count, *refs):
    pieces, outs = refs[:parts], refs[parts + 3 : parts + 3 + count]
    gate_ref, up_ref, down_ref = refs[parts : parts + 3]
    rows, acc = refs[parts + 3 + count :]
    size, out_size = pieces[0].shape[0], outs[0].shape[0]
    step = pl.program_id(0)

    @pl.when(step == 0)
    def _():
        for k in range(parts):
            rows[k * size : (k + 1) * size] = pieces[k][...]

    term = swiglu_term(rows[...], gate_ref[0], up_ref[0], down_ref[0])

    @pl.when(step == 0)
    def _():
        acc[...] = term

    @pl.when((step > 0) & (step < pl.num_programs(0) - 1))
    def _():
        acc[...] += term

    @pl.when(step == pl.num_programs(0) - 1)
    def _():
        total = acc[...] + term
        for k in range(count):
            outs[k][...] = total[k * out_size : (k + 1) * out_size].astype(BF16)


def expert_rows(pieces, count, expert_gate, expert_up, expert_down):
    parts = len(pieces)
    size, width = pieces[0].shape
    out_size = parts * size // count
    hidden = expert_gate.shape[2]
    tile = hidden // 2
    out = jax.ShapeDtypeStruct((out_size, width), BF16)
    weights = [expert_gate, expert_up, expert_down]
    return pl.pallas_call(
        functools.partial(expert_kernel, parts, count),
        out_shape=[out] * count,
        grid=(2,),
        in_specs=[pl.BlockSpec((size, width), lambda i: (0, 0))] * parts
        + [
            pl.BlockSpec((1, width, tile), lambda i: (0, 0, i)),
            pl.BlockSpec((1, width, tile), lambda i: (0, 0, i)),
            pl.BlockSpec((1, tile, width), lambda i: (0, i, 0)),
        ],
        out_specs=[pl.BlockSpec((out_size, width), lambda i: (0, 0))] * count,
        scratch_shapes=[
            pltpu.VMEM((parts * size, width), BF16),
            pltpu.VMEM((parts * size, width), F32),
        ],
        cost_estimate=cost(2 * parts * size * 3 * width * hidden, weights),
        compiler_params=grant(20),
        name="expert_rows",
    )(*pieces, *weights)


def shared_kernel(rows_ref, stream_ref, gate_ref, up_ref, down_ref, out_ref):
    term = swiglu_term(rows_ref[...], gate_ref[...], up_ref[...], down_ref[...])

    @pl.when(pl.program_id(0) == 0)
    def _():
        out_ref[...] = stream_ref[...] + term

    @pl.when(pl.program_id(0) > 0)
    def _():
        out_ref[...] += term


def shared_rows(normed, stream, gate, up, down):
    rows, width = normed.shape
    hidden = gate.shape[1]
    tile = hidden // 2
    fixed = pl.BlockSpec((rows, width), lambda i: (0, 0))
    return pl.pallas_call(
        shared_kernel,
        out_shape=jax.ShapeDtypeStruct((rows, width), F32),
        grid=(2,),
        in_specs=[
            fixed,
            fixed,
            pl.BlockSpec((width, tile), lambda i: (0, i)),
            pl.BlockSpec((width, tile), lambda i: (0, i)),
            pl.BlockSpec((tile, width), lambda i: (i, 0)),
        ],
        out_specs=fixed,
        cost_estimate=cost(6 * rows * width * hidden, [gate, up, down]),
        compiler_params=grant(12),
        name="shared_rows",
    )(normed, stream, gate, up, down)


def combine_kernel(parts, chips, *refs):
    pieces, table = refs[:parts], refs[parts]
    full_ref, short_ref, high, low, rows = refs[parts + 1 :]
    size = pieces[0].shape[0]
    tokens = table.shape[1]
    slots = lax.broadcasted_iota(jnp.int32, (size, tokens), 0).astype(F32)
    for k in range(parts):
        at = slice(k * size, (k + 1) * size)
        row = (k % 2) * chips + k // 2
        named = table[row : row + 1] == slots
        weight = jnp.where(named, table[2 * chips + row : 2 * chips + row + 1], 0.0)
        top = weight.astype(BF16)
        high[at] = top
        low[at] = (weight - top.astype(F32)).astype(BF16)
        rows[at] = pieces[k][...]
    contract = (((0,), (0,)), ((), ()))
    total = lax.dot_general(high[...], rows[...], contract, preferred_element_type=F32)
    total += lax.dot_general(low[...], rows[...], contract, preferred_element_type=F32)
    full_ref[...] = total
    short_ref[...] = total.astype(BF16)


def combine(pieces, table):
    parts = len(pieces)
    size, width = pieces[0].shape
    tokens = table.shape[1]
    whole = pl.BlockSpec(memory_space=pltpu.VMEM)
    out_shape = [
        jax.ShapeDtypeStruct((tokens, width), F32),
        jax.ShapeDtypeStruct((tokens, width), BF16),
    ]
    return pl.pallas_call(
        functools.partial(combine_kernel, parts, parts // 2),
        out_shape=out_shape,
        in_specs=[whole] * (parts + 1),
        out_specs=[whole] * 2,
        scratch_shapes=[
            pltpu.VMEM((parts * size, tokens), BF16),
            pltpu.VMEM((parts * size, tokens), BF16),
            pltpu.VMEM((parts * size, width), BF16),
        ],
        cost_estimate=cost(4 * parts * size * tokens * width, out_shape),
        compiler_params=grant(8),
        name="combine_rows",
    )(*pieces, table)


def ring(count, distance):
    order = [p ^ (p >> 1) for p in range(count)]
    return [(order[p], order[(p + distance) % count]) for p in range(count)]


def gather_ring(own, count):
    if count != 4:
        return [own] + [lax.ppermute(own, "z", ring(count, j)) for j in range(1, count)]
    one = lax.ppermute(own, "z", ring(4, 1))
    two = lax.ppermute(one, "z", ring(4, 1))
    three = lax.ppermute(own, "z", ring(4, -1))
    return [own, one, two, three]


def exchange(pieces, axes):
    count = len(pieces)
    moved = [lax.ppermute(pieces[k], axes, flips(count, k)) for k in range(1, count)]
    return [pieces[0]] + moved


def gate_tables(routes, route_weights, experts, rank, pair_rank):
    gate_values = route_weights / jnp.sum(route_weights, axis=1, keepdims=True) * 2.5
    hits = routes.T[:, None, :] == experts
    gates_of = jnp.sum(jnp.where(hits, gate_values.T[:, None, :], 0.0), axis=0)
    table = jnp.concatenate([rank, gates_of.reshape(rank.shape), pair_rank], axis=1)
    count = rank.shape[0]
    return [table[0]] + [lax.ppermute(table[j], "z", ring(count, j)) for j in range(1, count)]


def layer(
    out_gate,
    in_gate,
    conv_values,
    conv_taps,
    mix_gain,
    out_proj,
    residual,
    ffn_gain,
    routes,
    route_weights,
    shared_gate,
    shared_up,
    shared_down,
    expert_gate,
    expert_up,
    expert_down,
):
    z_count, tp_count = lax.axis_size("z"), lax.axis_size(TP)
    chips = lax.axis_size(CHIPS)
    z_index, tp_index = lax.axis_index("z"), lax.axis_index(TP)
    chip_index, core_index = lax.axis_index(CHIPS), lax.axis_index("c")

    back = conv_taps.shape[0] - 1
    length = conv_values.shape[0]
    tail = in_gate[length - back :].astype(F32) * conv_values[length - back :].astype(F32)
    halo = from_behind(tail, 1)
    me = tp_index.reshape(1).astype(jnp.int32)
    seq = lax.axis_index(SEQ).reshape(1).astype(jnp.int32)
    blocks, head = filter_rows(me, out_gate, in_gate, conv_values, conv_taps, tp_count)
    blocks = mend_rows(me, seq, blocks, head, back, halo)
    pieces = exchange(blocks, TP)
    late = (routes, mix_gain, pieces[1])
    routes, mix_gain, _ = lax.optimization_barrier(late)

    row_count, top_count = routes.shape
    capacity = max(2, 4 * row_count * top_count // (6 * z_count * chips))
    place = z_index ^ (z_index >> 1) ^ (z_index >> 2)
    later = (jnp.arange(z_count, dtype=jnp.int32) + place) & (z_count - 1)
    layers = later ^ (later >> 1)
    cores = jnp.arange(2, dtype=jnp.int32) ^ core_index
    places = jnp.arange(chips, dtype=jnp.int32) ^ chip_index
    experts = (layers[:, None, None] * chips + places) * 2 + cores[:, None]
    experts = experts.reshape(-1)[None, :, None]
    named = jnp.any(routes.T[:, None, :] == experts, axis=0)
    steps = jnp.arange(row_count, dtype=jnp.int32)
    earlier = (steps[:, None] < steps[None, :]).astype(BF16)
    rank = jnp.dot(named.astype(BF16), earlier, preferred_element_type=F32)
    rank = jnp.where(named, rank, -1.0)
    out_proj, rank = lax.optimization_barrier((out_proj, rank))
    rank = rank.reshape(z_count, 2 * chips, row_count)
    pair_rank = lax.ppermute(rank[:, chips:], "c", flips(2, 1))
    out_proj = fetch(out_proj)

    stream, normed = mix_project(me, pieces, mix_gain, out_proj, residual, ffn_gain)

    sources = gather_ring(normed, z_count)
    weights = (expert_gate, expert_up, expert_down)
    tables, results = [], []
    for j in range(z_count):
        pair = lax.ppermute(sources[j], "c", flips(2, 1))
        table = tables[j] if j else jnp.concatenate([rank[0], pair_rank[0]])
        outgoing = outgoing_rows(sources[j], pair, table, chips, capacity)
        if j == 0:
            tables = gate_tables(routes, route_weights, experts, rank, pair_rank)
        arrived = exchange(outgoing, CHIPS)
        results.append(expert_rows(arrived, 2 * chips, *weights))

    base = shared_rows(normed, stream, shared_gate, shared_up, shared_down)

    partial, short = [None] * z_count, [None] * z_count
    for j in reversed(range(z_count)):
        returned = exchange(results[j], PLANE)
        partial[j], short[j] = combine(returned, tables[j])

    if z_count == 4:

        def hop(block, distance):
            route = ring(4, distance)
            return lax.ppermute(block.astype(BF16), "z", route).astype(F32)

        far = hop(short[2], -1)
        last = hop(far + partial[1], -1)
        routed = partial[0] + hop(short[3], 1) + last
    else:
        routed = partial[0]
        for j in range(1, z_count):
            routed = routed + lax.ppermute(short[j], "z", ring(z_count, -j))
    return (base + routed).astype(BF16)


def solution(mesh):
    sp_count, tp_count = mesh.shape["sp"], mesh.shape["tp"]
    z_count = 1 << -(-(sp_count.bit_length() - 1) // 2)
    every = SEQ + TP
    split = Mesh(
        mesh.devices.reshape(z_count, sp_count // z_count, tp_count // 2, 2), every
    )
    in_specs = (
        P(SEQ, TP),
        P(SEQ, TP),
        P(SEQ, TP),
        P(None, TP),
        P(),
        P(),
        P(every, None),
        P(),
        P(every, None),
        P(every, None),
        P(),
        P(),
        P(),
        P(every, None, None),
        P(every, None, None),
        P(every, None, None),
    )
    return jax.shard_map(
        layer, mesh=split, in_specs=in_specs, out_specs=P(every, None), check_vma=False
    )
```

```python
import functools

import jax
import jax.numpy as jnp
from jax import lax
from jax.experimental import pallas as pl
from jax.experimental.pallas import tpu as pltpu
from jax.sharding import Mesh, PartitionSpec as P


SEQ, TP, CHIPS, PLANE = ("z", "x"), ("y", "c"), ("x", "y"), ("x", "y", "c")
BF16, F32 = jnp.bfloat16, jnp.float32


def flips(count, distance):
    return [(i, i ^ distance) for i in range(count)]


def from_behind(block, distance):
    count = lax.axis_size(SEQ)
    route = [((i - distance) % count, i) for i in range(count)]
    return lax.ppermute(block, SEQ, route)


def grant(mib):
    return pltpu.CompilerParams(vmem_limit_bytes=mib << 20)


def cost(flops, arrays):
    size = sum(a.size * a.dtype.itemsize for a in arrays)
    return pl.CostEstimate(flops=flops, bytes_accessed=size, transcendentals=0)


def filter_kernel(parts, back, me_ref, gate_ref, in_ref, val_ref, taps_ref, *rest):
    outs, head_ref, scratch = rest[:parts], rest[parts], rest[parts + 1]
    length = val_ref.shape[0]
    rows = length // parts
    scratch[0:8] = jnp.zeros((8, scratch.shape[1]), F32)
    scratch[8:] = in_ref[...].astype(F32) * val_ref[...].astype(F32)
    me = me_ref[0]
    for k in range(parts):
        start = pl.multiple_of((me ^ k) * rows, 16)
        window = scratch[pl.ds(start, rows + 8)]
        total = taps_ref[0:1] * window[8 - back : 8 - back + rows]
        for offset in range(1, back + 1):
            first = 8 - back + offset
            total = total + taps_ref[offset : offset + 1] * window[first : first + rows]
        outs[k][...] = (gate_ref[pl.ds(start, rows)].astype(F32) * total).astype(BF16)
    window = scratch[0:24]
    total = taps_ref[0:1] * window[8 - back : 24 - back]
    for offset in range(1, back + 1):
        first = 8 - back + offset
        total = total + taps_ref[offset : offset + 1] * window[first : first + 16]
    head_ref[0:16] = total
    head_ref[16:32] = gate_ref[0:16].astype(F32)
    head_ref[32 : 33 + back] = taps_ref[...]


def filter_rows(me, out_gate, in_gate, conv_values, conv_taps, parts):
    length, channels = conv_values.shape
    out = jax.ShapeDtypeStruct((length // parts, channels), BF16)
    whole = pl.BlockSpec(memory_space=pltpu.VMEM)
    *blocks, head = pl.pallas_call(
        functools.partial(filter_kernel, parts, conv_taps.shape[0] - 1),
        out_shape=[pltpu.VMEM(out.shape, BF16)] * parts + [pltpu.VMEM((40, channels), F32)],
        in_specs=[pl.BlockSpec(memory_space=pltpu.SMEM)] + [whole] * 4,
        out_specs=[whole] * (parts + 1),
        scratch_shapes=[pltpu.VMEM((length + 8, channels), F32)],
        cost_estimate=cost(1 << 20, [out_gate, in_gate, conv_values]),
        name="filter_rows",
    )(me, out_gate, in_gate, conv_values, conv_taps)
    return blocks, head


def mend_kernel(parts, back, me_ref, seq_ref, head_ref, halo_ref, *refs):
    outs = refs[parts:]
    channels = head_ref.shape[1]
    row = lax.broadcasted_iota(jnp.int32, (16, channels), 0)
    total = head_ref[0:16]
    for offset in range(back):
        for at_row in range(back - offset):
            tap = head_ref[32 + offset : 33 + offset]
            term = tap * halo_ref[at_row + offset : at_row + offset + 1]
            total = total + jnp.where((row == at_row) & (seq_ref[0] > 0), term, 0.0)
    fresh = (head_ref[16:32] * total).astype(BF16)
    for k in range(parts):

        @pl.when(me_ref[0] == k)
        def _(k=k):
            outs[k][0:16] = fresh


def mend_rows(me, seq, blocks, head, back, halo):
    parts = len(blocks)
    whole = pl.BlockSpec(memory_space=pltpu.VMEM)
    return pl.pallas_call(
        functools.partial(mend_kernel, parts, back),
        out_shape=[pltpu.VMEM(blocks[0].shape, BF16)] * parts,
        in_specs=[pl.BlockSpec(memory_space=pltpu.SMEM)] * 2 + [whole] * (2 + parts),
        out_specs=[whole] * parts,
        input_output_aliases={4 + k: k for k in range(parts)},
        cost_estimate=cost(1 << 20, blocks),
        compiler_params=grant(8),
        name="mend_rows",
    )(me, seq, head, halo, *blocks)


def fetch_kernel(from_ref, to_ref, sem):
    copy = pltpu.make_async_copy(from_ref, to_ref, sem)
    copy.start()
    copy.wait()


def fetch(array):
    return pl.pallas_call(
        fetch_kernel,
        out_shape=pltpu.VMEM(array.shape, array.dtype),
        in_specs=[pl.BlockSpec(memory_space=pltpu.HBM)],
        out_specs=pl.BlockSpec(memory_space=pltpu.VMEM),
        scratch_shapes=[pltpu.SemaphoreType.DMA],
        cost_estimate=cost(1 << 20, [array]),
        compiler_params=grant(54),
        name="fetch_rows",
    )(array)


def mix_kernel(parts, me_ref, *refs):
    pieces = refs[:parts]
    mix_gain, out_proj, residual, ffn_gain, stream_ref, normed_ref, acc, squares = refs[parts:]
    step = pl.program_id(0)

    @pl.when(step == 0)
    def _():
        acc[...] = jnp.zeros_like(acc)
        squares[...] = jnp.zeros_like(squares)

    for k in range(parts):

        @pl.when(step == k)
        def _(k=k):
            values = pieces[k][...].astype(F32)
            squares[...] += jnp.sum(values * values, axis=1, keepdims=True)
            scaled = (values * mix_gain[...].reshape(1, -1)).astype(BF16)
            acc[...] += jnp.dot(scaled, out_proj[...], preferred_element_type=F32)

    @pl.when(step == parts - 1)
    def _():
        channels = parts * pieces[0].shape[1]
        inverse = lax.rsqrt(squares[...] / channels + 1e-06)
        stream = residual[...].astype(F32) + acc[...] * inverse
        stream_ref[...] = stream
        mean = jnp.mean(stream * stream, axis=1, keepdims=True)
        normed_ref[...] = (stream * lax.rsqrt(mean + 1e-06) * ffn_gain[...]).astype(BF16)


def mix_project(me, pieces, mix_gain, out_proj, residual, ffn_gain):
    parts = len(pieces)
    rows, channels = pieces[0].shape
    width = out_proj.shape[1]
    fixed = lambda shape: pl.BlockSpec(shape, lambda i, me_ref: (0,) * len(shape))
    if channels % 128:
        gain = mix_gain.reshape(parts, 1, channels)
        gain_spec = pl.BlockSpec((1, 1, channels), lambda i, me_ref: (me_ref[0] ^ i, 0, 0))
    else:
        gain = mix_gain[None]
        gain_spec = pl.BlockSpec((1, channels), lambda i, me_ref: (0, me_ref[0] ^ i))
    out_shape = [
        pltpu.HBM((rows, width), F32),
        jax.ShapeDtypeStruct((rows, width), BF16),
    ]
    grid_spec = pltpu.PrefetchScalarGridSpec(
        num_scalar_prefetch=1,
        grid=(parts,),
        in_specs=[fixed((rows, channels))] * parts
        + [
            gain_spec,
            pl.BlockSpec((channels, width), lambda i, me_ref: (me_ref[0] ^ i, 0)),
            fixed((rows, width)),
            fixed((1, width)),
        ],
        out_specs=[fixed((rows, width))] * 2,
        scratch_shapes=[pltpu.VMEM((rows, width), F32), pltpu.VMEM((rows, 1), F32)],
    )
    return pl.pallas_call(
        functools.partial(mix_kernel, parts),
        out_shape=out_shape,
        grid_spec=grid_spec,
        cost_estimate=cost(2 * rows * out_proj.size, [out_proj, residual]),
        compiler_params=grant(14),
        name="mix_project",
    )(me, *pieces, gain, out_proj, residual, ffn_gain[None])


def send_kernel(chips, base, own_ref, pair_ref, table_ref, *outs):
    size = outs[0].shape[0] // 2
    tokens = own_ref.shape[0]
    slots = lax.broadcasted_iota(jnp.int32, (size, tokens), 0).astype(F32)
    for side, (ref, first) in enumerate(((own_ref, 0), (pair_ref, base))):
        pick = jnp.concatenate(
            [
                (table_ref[first + k : first + k + 1] == slots).astype(F32).astype(BF16)
                for k in range(chips)
            ]
        )
        rows = jnp.dot(pick, ref[...], preferred_element_type=F32).astype(BF16)
        for k in range(chips):
            outs[k][side * size : (side + 1) * size] = rows[k * size : (k + 1) * size]


def outgoing_rows(own, pair, table, chips, capacity):
    tokens, width = own.shape
    whole = pl.BlockSpec(memory_space=pltpu.VMEM)
    out_shape = [jax.ShapeDtypeStruct((2 * capacity, width), BF16)] * chips
    return pl.pallas_call(
        functools.partial(send_kernel, chips, table.shape[0] - chips),
        out_shape=out_shape,
        in_specs=[whole] * 3,
        out_specs=[whole] * chips,
        cost_estimate=cost(4 * chips * capacity * tokens * width, [own, pair] + out_shape),
        compiler_params=grant(6),
        name="outgoing_rows",
    )(own, pair, table)


def swiglu_term(rows, gate_ref, up_ref, down_ref):
    gate_part = jnp.dot(rows, gate_ref, preferred_element_type=F32)
    up_part = jnp.dot(rows, up_ref, preferred_element_type=F32)
    hidden = (gate_part / (1.0 + jnp.exp(-gate_part)) * up_part).astype(BF16)
    return jnp.dot(hidden, down_ref, preferred_element_type=F32)


def expert_kernel(parts, count, *refs):
    pieces, outs = refs[:parts], refs[parts + 3 : parts + 3 + count]
    gate_ref, up_ref, down_ref = refs[parts : parts + 3]
    rows, acc = refs[parts + 3 + count :]
    size, out_size = pieces[0].shape[0], outs[0].shape[0]
    step = pl.program_id(0)

    @pl.when(step == 0)
    def _():
        for k in range(parts):
            rows[k * size : (k + 1) * size] = pieces[k][...]

    term = swiglu_term(rows[...], gate_ref[0], up_ref[0], down_ref[0])

    @pl.when(step == 0)
    def _():
        acc[...] = term

    @pl.when((step > 0) & (step < pl.num_programs(0) - 1))
    def _():
        acc[...] += term

    @pl.when(step == pl.num_programs(0) - 1)
    def _():
        total = acc[...] + term
        for k in range(count):
            outs[k][...] = total[k * out_size : (k + 1) * out_size].astype(BF16)


def expert_rows(pieces, count, expert_gate, expert_up, expert_down):
    parts = len(pieces)
    size, width = pieces[0].shape
    out_size = parts * size // count
    hidden = expert_gate.shape[2]
    tile = hidden // 2
    out = jax.ShapeDtypeStruct((out_size, width), BF16)
    weights = [expert_gate, expert_up, expert_down]
    return pl.pallas_call(
        functools.partial(expert_kernel, parts, count),
        out_shape=[out] * count,
        grid=(2,),
        in_specs=[pl.BlockSpec((size, width), lambda i: (0, 0))] * parts
        + [
            pl.BlockSpec((1, width, tile), lambda i: (0, 0, i)),
            pl.BlockSpec((1, width, tile), lambda i: (0, 0, i)),
            pl.BlockSpec((1, tile, width), lambda i: (0, i, 0)),
        ],
        out_specs=[pl.BlockSpec((out_size, width), lambda i: (0, 0))] * count,
        scratch_shapes=[
            pltpu.VMEM((parts * size, width), BF16),
            pltpu.VMEM((parts * size, width), F32),
        ],
        cost_estimate=cost(2 * parts * size * 3 * width * hidden, weights),
        compiler_params=grant(20),
        name="expert_rows",
    )(*pieces, *weights)


def shared_kernel(rows_ref, stream_ref, gate_ref, up_ref, down_ref, out_ref):
    term = swiglu_term(rows_ref[...], gate_ref[...], up_ref[...], down_ref[...])

    @pl.when(pl.program_id(0) == 0)
    def _():
        out_ref[...] = stream_ref[...] + term

    @pl.when(pl.program_id(0) > 0)
    def _():
        out_ref[...] += term


def shared_rows(normed, stream, gate, up, down):
    rows, width = normed.shape
    hidden = gate.shape[1]
    tile = hidden // 2
    fixed = pl.BlockSpec((rows, width), lambda i: (0, 0))
    return pl.pallas_call(
        shared_kernel,
        out_shape=jax.ShapeDtypeStruct((rows, width), F32),
        grid=(2,),
        in_specs=[
            fixed,
            fixed,
            pl.BlockSpec((width, tile), lambda i: (0, i)),
            pl.BlockSpec((width, tile), lambda i: (0, i)),
            pl.BlockSpec((tile, width), lambda i: (i, 0)),
        ],
        out_specs=fixed,
        cost_estimate=cost(6 * rows * width * hidden, [gate, up, down]),
        compiler_params=grant(12),
        name="shared_rows",
    )(normed, stream, gate, up, down)


def combine_kernel(parts, chips, *refs):
    pieces, table = refs[:parts], refs[parts]
    full_ref, short_ref, high, low, rows = refs[parts + 1 :]
    size = pieces[0].shape[0]
    tokens = table.shape[1]
    slots = lax.broadcasted_iota(jnp.int32, (size, tokens), 0).astype(F32)
    for k in range(parts):
        at = slice(k * size, (k + 1) * size)
        row = (k % 2) * chips + k // 2
        named = table[row : row + 1] == slots
        weight = jnp.where(named, table[2 * chips + row : 2 * chips + row + 1], 0.0)
        top = weight.astype(BF16)
        high[at] = top
        low[at] = (weight - top.astype(F32)).astype(BF16)
        rows[at] = pieces[k][...]
    contract = (((0,), (0,)), ((), ()))
    total = lax.dot_general(high[...], rows[...], contract, preferred_element_type=F32)
    total += lax.dot_general(low[...], rows[...], contract, preferred_element_type=F32)
    full_ref[...] = total
    short_ref[...] = total.astype(BF16)


def combine(pieces, table):
    parts = len(pieces)
    size, width = pieces[0].shape
    tokens = table.shape[1]
    whole = pl.BlockSpec(memory_space=pltpu.VMEM)
    out_shape = [
        jax.ShapeDtypeStruct((tokens, width), F32),
        jax.ShapeDtypeStruct((tokens, width), BF16),
    ]
    return pl.pallas_call(
        functools.partial(combine_kernel, parts, parts // 2),
        out_shape=out_shape,
        in_specs=[whole] * (parts + 1),
        out_specs=[whole] * 2,
        scratch_shapes=[
            pltpu.VMEM((parts * size, tokens), BF16),
            pltpu.VMEM((parts * size, tokens), BF16),
            pltpu.VMEM((parts * size, width), BF16),
        ],
        cost_estimate=cost(4 * parts * size * tokens * width, out_shape),
        compiler_params=grant(8),
        name="combine_rows",
    )(*pieces, table)


def ring(count, distance):
    order = [p ^ (p >> 1) for p in range(count)]
    return [(order[p], order[(p + distance) % count]) for p in range(count)]


def gather_ring(own, count):
    if count != 4:
        return [own] + [lax.ppermute(own, "z", ring(count, j)) for j in range(1, count)]
    one = lax.ppermute(own, "z", ring(4, 1))
    two = lax.ppermute(one, "z", ring(4, 1))
    three = lax.ppermute(own, "z", ring(4, -1))
    return [own, one, two, three]


def exchange(pieces, axes):
    count = len(pieces)
    moved = [lax.ppermute(pieces[k], axes, flips(count, k)) for k in range(1, count)]
    return [pieces[0]] + moved


def gate_tables(routes, route_weights, experts, rank, pair_rank):
    gate_values = route_weights / jnp.sum(route_weights, axis=1, keepdims=True) * 2.5
    hits = routes.T[:, None, :] == experts
    gates_of = jnp.sum(jnp.where(hits, gate_values.T[:, None, :], 0.0), axis=0)
    table = jnp.concatenate([rank, gates_of.reshape(rank.shape), pair_rank], axis=1)
    count = rank.shape[0]
    return [table[0]] + [lax.ppermute(table[j], "z", ring(count, j)) for j in range(1, count)]


def layer(
    out_gate,
    in_gate,
    conv_values,
    conv_taps,
    mix_gain,
    out_proj,
    residual,
    ffn_gain,
    routes,
    route_weights,
    shared_gate,
    shared_up,
    shared_down,
    expert_gate,
    expert_up,
    expert_down,
):
    z_count, tp_count = lax.axis_size("z"), lax.axis_size(TP)
    chips = lax.axis_size(CHIPS)
    z_index, tp_index = lax.axis_index("z"), lax.axis_index(TP)
    chip_index, core_index = lax.axis_index(CHIPS), lax.axis_index("c")

    back = conv_taps.shape[0] - 1
    length = conv_values.shape[0]
    tail = in_gate[length - back :].astype(F32) * conv_values[length - back :].astype(F32)
    halo = from_behind(tail, 1)
    me = tp_index.reshape(1).astype(jnp.int32)
    seq = lax.axis_index(SEQ).reshape(1).astype(jnp.int32)
    blocks, head = filter_rows(me, out_gate, in_gate, conv_values, conv_taps, tp_count)
    blocks = mend_rows(me, seq, blocks, head, back, halo)
    pieces = exchange(blocks, TP)
    late = (routes, mix_gain, pieces[1])
    routes, mix_gain, _ = lax.optimization_barrier(late)

    row_count, top_count = routes.shape
    capacity = max(2, 4 * row_count * top_count // (6 * z_count * chips))
    place = z_index ^ (z_index >> 1) ^ (z_index >> 2)
    later = (jnp.arange(z_count, dtype=jnp.int32) + place) & (z_count - 1)
    layers = later ^ (later >> 1)
    cores = jnp.arange(2, dtype=jnp.int32) ^ core_index
    places = jnp.arange(chips, dtype=jnp.int32) ^ chip_index
    experts = (layers[:, None, None] * chips + places) * 2 + cores[:, None]
    experts = experts.reshape(-1)[None, :, None]
    named = jnp.any(routes.T[:, None, :] == experts, axis=0)
    steps = jnp.arange(row_count, dtype=jnp.int32)
    earlier = (steps[:, None] < steps[None, :]).astype(BF16)
    rank = jnp.dot(named.astype(BF16), earlier, preferred_element_type=F32)
    rank = jnp.where(named, rank, -1.0)
    out_proj, rank = lax.optimization_barrier((out_proj, rank))
    rank = rank.reshape(z_count, 2 * chips, row_count)
    pair_rank = lax.ppermute(rank[:, chips:], "c", flips(2, 1))
    out_proj = fetch(out_proj)

    stream, normed = mix_project(me, pieces, mix_gain, out_proj, residual, ffn_gain)

    sources = gather_ring(normed, z_count)
    weights = (expert_gate, expert_up, expert_down)
    tables, results = [], []
    for j in range(z_count):
        pair = lax.ppermute(sources[j], "c", flips(2, 1))
        table = tables[j] if j else jnp.concatenate([rank[0], pair_rank[0]])
        outgoing = outgoing_rows(sources[j], pair, table, chips, capacity)
        if j == 0:
            tables = gate_tables(routes, route_weights, experts, rank, pair_rank)
        arrived = exchange(outgoing, CHIPS)
        results.append(expert_rows(arrived, 2 * chips, *weights))

    base = shared_rows(normed, stream, shared_gate, shared_up, shared_down)

    partial, short = [None] * z_count, [None] * z_count
    for j in reversed(range(z_count)):
        returned = exchange(results[j], PLANE)
        partial[j], short[j] = combine(returned, tables[j])

    if z_count == 4:

        def hop(block, distance):
            route = ring(4, distance)
            return lax.ppermute(block.astype(BF16), "z", route).astype(F32)

        back = hop(short[1], -1)
        ahead = hop(short[2], 1)
        ahead = hop(ahead + partial[3], 1)
        routed = partial[0] + back + ahead
    else:
        routed = partial[0]
        for j in range(1, z_count):
            routed = routed + lax.ppermute(short[j], "z", ring(z_count, -j))
    return (base + routed).astype(BF16)


def solution(mesh):
    sp_count, tp_count = mesh.shape["sp"], mesh.shape["tp"]
    z_count = 1 << -(-(sp_count.bit_length() - 1) // 2)
    every = SEQ + TP
    split = Mesh(
        mesh.devices.reshape(z_count, sp_count // z_count, tp_count // 2, 2), every
    )
    in_specs = (
        P(SEQ, TP),
        P(SEQ, TP),
        P(SEQ, TP),
        P(None, TP),
        P(),
        P(),
        P(every, None),
        P(),
        P(every, None),
        P(every, None),
        P(),
        P(),
        P(),
        P(every, None, None),
        P(every, None, None),
        P(every, None, None),
    )
    return jax.shard_map(
        layer, mesh=split, in_specs=in_specs, out_specs=P(every, None), check_vma=False
    )
```

```python
import functools

import jax
import jax.numpy as jnp
from jax import lax
from jax.experimental import pallas as pl
from jax.experimental.pallas import tpu as pltpu
from jax.sharding import Mesh, PartitionSpec as P


SEQ, TP, CHIPS, PLANE = ("z", "x"), ("y", "c"), ("x", "y"), ("x", "y", "c")
BF16, F32 = jnp.bfloat16, jnp.float32


def flips(count, distance):
    return [(i, i ^ distance) for i in range(count)]


def from_behind(block, distance):
    count = lax.axis_size(SEQ)
    route = [((i - distance) % count, i) for i in range(count)]
    return lax.ppermute(block, SEQ, route)


def grant(mib):
    return pltpu.CompilerParams(vmem_limit_bytes=mib << 20)


def cost(flops, arrays):
    size = sum(a.size * a.dtype.itemsize for a in arrays)
    return pl.CostEstimate(flops=flops, bytes_accessed=size, transcendentals=0)


def filter_kernel(parts, back, me_ref, gate_ref, in_ref, val_ref, taps_ref, *rest):
    outs, head_ref, scratch = rest[:parts], rest[parts], rest[parts + 1]
    length = val_ref.shape[0]
    rows = length // parts
    scratch[0:8] = jnp.zeros((8, scratch.shape[1]), F32)
    scratch[8:] = in_ref[...].astype(F32) * val_ref[...].astype(F32)
    me = me_ref[0]
    for k in range(parts):
        start = pl.multiple_of((me ^ k) * rows, 16)
        window = scratch[pl.ds(start, rows + 8)]
        total = taps_ref[0:1] * window[8 - back : 8 - back + rows]
        for offset in range(1, back + 1):
            first = 8 - back + offset
            total = total + taps_ref[offset : offset + 1] * window[first : first + rows]
        outs[k][...] = (gate_ref[pl.ds(start, rows)].astype(F32) * total).astype(BF16)
    window = scratch[0:24]
    total = taps_ref[0:1] * window[8 - back : 24 - back]
    for offset in range(1, back + 1):
        first = 8 - back + offset
        total = total + taps_ref[offset : offset + 1] * window[first : first + 16]
    head_ref[0:16] = total
    head_ref[16:32] = gate_ref[0:16].astype(F32)
    head_ref[32 : 33 + back] = taps_ref[...]


def filter_rows(me, out_gate, in_gate, conv_values, conv_taps, parts):
    length, channels = conv_values.shape
    out = jax.ShapeDtypeStruct((length // parts, channels), BF16)
    whole = pl.BlockSpec(memory_space=pltpu.VMEM)
    *blocks, head = pl.pallas_call(
        functools.partial(filter_kernel, parts, conv_taps.shape[0] - 1),
        out_shape=[pltpu.VMEM(out.shape, BF16)] * parts + [pltpu.VMEM((40, channels), F32)],
        in_specs=[pl.BlockSpec(memory_space=pltpu.SMEM)] + [whole] * 4,
        out_specs=[whole] * (parts + 1),
        scratch_shapes=[pltpu.VMEM((length + 8, channels), F32)],
        cost_estimate=cost(1 << 20, [out_gate, in_gate, conv_values]),
        name="filter_rows",
    )(me, out_gate, in_gate, conv_values, conv_taps)
    return blocks, head


def mend_kernel(parts, back, me_ref, seq_ref, head_ref, halo_ref, *refs):
    outs = refs[parts:]
    channels = head_ref.shape[1]
    row = lax.broadcasted_iota(jnp.int32, (16, channels), 0)
    total = head_ref[0:16]
    for offset in range(back):
        for at_row in range(back - offset):
            tap = head_ref[32 + offset : 33 + offset]
            term = tap * halo_ref[at_row + offset : at_row + offset + 1]
            total = total + jnp.where((row == at_row) & (seq_ref[0] > 0), term, 0.0)
    fresh = (head_ref[16:32] * total).astype(BF16)
    for k in range(parts):

        @pl.when(me_ref[0] == k)
        def _(k=k):
            outs[k][0:16] = fresh


def mend_rows(me, seq, blocks, head, back, halo):
    parts = len(blocks)
    whole = pl.BlockSpec(memory_space=pltpu.VMEM)
    return pl.pallas_call(
        functools.partial(mend_kernel, parts, back),
        out_shape=[pltpu.VMEM(blocks[0].shape, BF16)] * parts,
        in_specs=[pl.BlockSpec(memory_space=pltpu.SMEM)] * 2 + [whole] * (2 + parts),
        out_specs=[whole] * parts,
        input_output_aliases={4 + k: k for k in range(parts)},
        cost_estimate=cost(1 << 20, blocks),
        compiler_params=grant(8),
        name="mend_rows",
    )(me, seq, head, halo, *blocks)


def fetch_kernel(from_ref, to_ref, sems):
    rows = from_ref.shape[0] // 4
    copies = []
    for k in range(4):
        part = pl.ds(k * rows, rows)
        copies.append(pltpu.make_async_copy(from_ref.at[part], to_ref.at[part], sems.at[k]))
    for copy in copies:
        copy.start()
    for copy in copies:
        copy.wait()


def fetch(array):
    return pl.pallas_call(
        fetch_kernel,
        out_shape=pltpu.VMEM(array.shape, array.dtype),
        in_specs=[pl.BlockSpec(memory_space=pltpu.HBM)],
        out_specs=pl.BlockSpec(memory_space=pltpu.VMEM),
        scratch_shapes=[pltpu.SemaphoreType.DMA((4,))],
        cost_estimate=cost(1 << 20, [array]),
        compiler_params=grant(54),
        name="fetch_rows",
    )(array)


def mix_kernel(parts, me_ref, *refs):
    pieces = refs[:parts]
    mix_gain, out_proj, residual, ffn_gain, stream_ref, normed_ref, acc, squares = refs[parts:]
    step = pl.program_id(0)

    @pl.when(step == 0)
    def _():
        acc[...] = jnp.zeros_like(acc)
        squares[...] = jnp.zeros_like(squares)

    for k in range(parts):

        @pl.when(step == k)
        def _(k=k):
            values = pieces[k][...].astype(F32)
            squares[...] += jnp.sum(values * values, axis=1, keepdims=True)
            scaled = (values * mix_gain[...].reshape(1, -1)).astype(BF16)
            acc[...] += jnp.dot(scaled, out_proj[...], preferred_element_type=F32)

    @pl.when(step == parts - 1)
    def _():
        channels = parts * pieces[0].shape[1]
        inverse = lax.rsqrt(squares[...] / channels + 1e-06)
        stream = residual[...].astype(F32) + acc[...] * inverse
        stream_ref[...] = stream
        mean = jnp.mean(stream * stream, axis=1, keepdims=True)
        normed_ref[...] = (stream * lax.rsqrt(mean + 1e-06) * ffn_gain[...]).astype(BF16)


def mix_project(me, pieces, mix_gain, out_proj, residual, ffn_gain):
    parts = len(pieces)
    rows, channels = pieces[0].shape
    width = out_proj.shape[1]
    fixed = lambda shape: pl.BlockSpec(shape, lambda i, me_ref: (0,) * len(shape))
    if channels % 128:
        gain = mix_gain.reshape(parts, 1, channels)
        gain_spec = pl.BlockSpec((1, 1, channels), lambda i, me_ref: (me_ref[0] ^ i, 0, 0))
    else:
        gain = mix_gain[None]
        gain_spec = pl.BlockSpec((1, channels), lambda i, me_ref: (0, me_ref[0] ^ i))
    out_shape = [
        pltpu.HBM((rows, width), F32),
        jax.ShapeDtypeStruct((rows, width), BF16),
    ]
    grid_spec = pltpu.PrefetchScalarGridSpec(
        num_scalar_prefetch=1,
        grid=(parts,),
        in_specs=[fixed((rows, channels))] * parts
        + [
            gain_spec,
            pl.BlockSpec((channels, width), lambda i, me_ref: (me_ref[0] ^ i, 0)),
            fixed((rows, width)),
            fixed((1, width)),
        ],
        out_specs=[fixed((rows, width))] * 2,
        scratch_shapes=[pltpu.VMEM((rows, width), F32), pltpu.VMEM((rows, 1), F32)],
    )
    return pl.pallas_call(
        functools.partial(mix_kernel, parts),
        out_shape=out_shape,
        grid_spec=grid_spec,
        cost_estimate=cost(2 * rows * out_proj.size, [out_proj, residual]),
        compiler_params=grant(14),
        name="mix_project",
    )(me, *pieces, gain, out_proj, residual, ffn_gain[None])


def send_kernel(chips, base, own_ref, pair_ref, table_ref, *outs):
    size = outs[0].shape[0] // 2
    tokens = own_ref.shape[0]
    slots = lax.broadcasted_iota(jnp.int32, (size, tokens), 0).astype(F32)
    for side, (ref, first) in enumerate(((own_ref, 0), (pair_ref, base))):
        pick = jnp.concatenate(
            [
                (table_ref[first + k : first + k + 1] == slots).astype(F32).astype(BF16)
                for k in range(chips)
            ]
        )
        rows = jnp.dot(pick, ref[...], preferred_element_type=F32).astype(BF16)
        for k in range(chips):
            outs[k][side * size : (side + 1) * size] = rows[k * size : (k + 1) * size]


def outgoing_rows(own, pair, table, chips, capacity):
    tokens, width = own.shape
    whole = pl.BlockSpec(memory_space=pltpu.VMEM)
    out_shape = [jax.ShapeDtypeStruct((2 * capacity, width), BF16)] * chips
    return pl.pallas_call(
        functools.partial(send_kernel, chips, table.shape[0] - chips),
        out_shape=out_shape,
        in_specs=[whole] * 3,
        out_specs=[whole] * chips,
        cost_estimate=cost(4 * chips * capacity * tokens * width, [own, pair] + out_shape),
        compiler_params=grant(6),
        name="outgoing_rows",
    )(own, pair, table)


def swiglu_term(rows, gate_ref, up_ref, down_ref):
    gate_part = jnp.dot(rows, gate_ref, preferred_element_type=F32)
    up_part = jnp.dot(rows, up_ref, preferred_element_type=F32)
    hidden = (gate_part / (1.0 + jnp.exp(-gate_part)) * up_part).astype(BF16)
    return jnp.dot(hidden, down_ref, preferred_element_type=F32)


def expert_kernel(parts, count, *refs):
    pieces, outs = refs[:parts], refs[parts + 3 : parts + 3 + count]
    gate_ref, up_ref, down_ref = refs[parts : parts + 3]
    rows, acc = refs[parts + 3 + count :]
    size, out_size = pieces[0].shape[0], outs[0].shape[0]
    step = pl.program_id(0)

    @pl.when(step == 0)
    def _():
        for k in range(parts):
            rows[k * size : (k + 1) * size] = pieces[k][...]

    term = swiglu_term(rows[...], gate_ref[0], up_ref[0], down_ref[0])

    @pl.when(step == 0)
    def _():
        acc[...] = term

    @pl.when((step > 0) & (step < pl.num_programs(0) - 1))
    def _():
        acc[...] += term

    @pl.when(step == pl.num_programs(0) - 1)
    def _():
        total = acc[...] + term
        for k in range(count):
            outs[k][...] = total[k * out_size : (k + 1) * out_size].astype(BF16)


def expert_rows(pieces, count, expert_gate, expert_up, expert_down):
    parts = len(pieces)
    size, width = pieces[0].shape
    out_size = parts * size // count
    hidden = expert_gate.shape[2]
    tile = hidden // 2
    out = jax.ShapeDtypeStruct((out_size, width), BF16)
    weights = [expert_gate, expert_up, expert_down]
    return pl.pallas_call(
        functools.partial(expert_kernel, parts, count),
        out_shape=[out] * count,
        grid=(2,),
        in_specs=[pl.BlockSpec((size, width), lambda i: (0, 0))] * parts
        + [
            pl.BlockSpec((1, width, tile), lambda i: (0, 0, i)),
            pl.BlockSpec((1, width, tile), lambda i: (0, 0, i)),
            pl.BlockSpec((1, tile, width), lambda i: (0, i, 0)),
        ],
        out_specs=[pl.BlockSpec((out_size, width), lambda i: (0, 0))] * count,
        scratch_shapes=[
            pltpu.VMEM((parts * size, width), BF16),
            pltpu.VMEM((parts * size, width), F32),
        ],
        cost_estimate=cost(2 * parts * size * 3 * width * hidden, weights),
        compiler_params=grant(20),
        name="expert_rows",
    )(*pieces, *weights)


def shared_kernel(rows_ref, stream_ref, gate_ref, up_ref, down_ref, out_ref):
    term = swiglu_term(rows_ref[...], gate_ref[...], up_ref[...], down_ref[...])

    @pl.when(pl.program_id(0) == 0)
    def _():
        out_ref[...] = stream_ref[...] + term

    @pl.when(pl.program_id(0) > 0)
    def _():
        out_ref[...] += term


def shared_rows(normed, stream, gate, up, down):
    rows, width = normed.shape
    hidden = gate.shape[1]
    tile = hidden // 2
    fixed = pl.BlockSpec((rows, width), lambda i: (0, 0))
    return pl.pallas_call(
        shared_kernel,
        out_shape=jax.ShapeDtypeStruct((rows, width), F32),
        grid=(2,),
        in_specs=[
            fixed,
            fixed,
            pl.BlockSpec((width, tile), lambda i: (0, i)),
            pl.BlockSpec((width, tile), lambda i: (0, i)),
            pl.BlockSpec((tile, width), lambda i: (i, 0)),
        ],
        out_specs=fixed,
        cost_estimate=cost(6 * rows * width * hidden, [gate, up, down]),
        compiler_params=grant(12),
        name="shared_rows",
    )(normed, stream, gate, up, down)


def combine_kernel(parts, chips, *refs):
    pieces, table = refs[:parts], refs[parts]
    full_ref, short_ref, high, low, rows = refs[parts + 1 :]
    size = pieces[0].shape[0]
    tokens = table.shape[1]
    slots = lax.broadcasted_iota(jnp.int32, (size, tokens), 0).astype(F32)
    for k in range(parts):
        at = slice(k * size, (k + 1) * size)
        row = (k % 2) * chips + k // 2
        named = table[row : row + 1] == slots
        weight = jnp.where(named, table[2 * chips + row : 2 * chips + row + 1], 0.0)
        top = weight.astype(BF16)
        high[at] = top
        low[at] = (weight - top.astype(F32)).astype(BF16)
        rows[at] = pieces[k][...]
    contract = (((0,), (0,)), ((), ()))
    total = lax.dot_general(high[...], rows[...], contract, preferred_element_type=F32)
    total += lax.dot_general(low[...], rows[...], contract, preferred_element_type=F32)
    full_ref[...] = total
    short_ref[...] = total.astype(BF16)


def combine(pieces, table):
    parts = len(pieces)
    size, width = pieces[0].shape
    tokens = table.shape[1]
    whole = pl.BlockSpec(memory_space=pltpu.VMEM)
    out_shape = [
        jax.ShapeDtypeStruct((tokens, width), F32),
        jax.ShapeDtypeStruct((tokens, width), BF16),
    ]
    return pl.pallas_call(
        functools.partial(combine_kernel, parts, parts // 2),
        out_shape=out_shape,
        in_specs=[whole] * (parts + 1),
        out_specs=[whole] * 2,
        scratch_shapes=[
            pltpu.VMEM((parts * size, tokens), BF16),
            pltpu.VMEM((parts * size, tokens), BF16),
            pltpu.VMEM((parts * size, width), BF16),
        ],
        cost_estimate=cost(4 * parts * size * tokens * width, out_shape),
        compiler_params=grant(8),
        name="combine_rows",
    )(*pieces, table)


def ring(count, distance):
    order = [p ^ (p >> 1) for p in range(count)]
    return [(order[p], order[(p + distance) % count]) for p in range(count)]


def gather_ring(own, count):
    if count != 4:
        return [own] + [lax.ppermute(own, "z", ring(count, j)) for j in range(1, count)]
    one = lax.ppermute(own, "z", ring(4, 1))
    two = lax.ppermute(one, "z", ring(4, 1))
    three = lax.ppermute(own, "z", ring(4, -1))
    return [own, one, two, three]


def exchange(pieces, axes):
    count = len(pieces)
    moved = [lax.ppermute(pieces[k], axes, flips(count, k)) for k in range(1, count)]
    return [pieces[0]] + moved


def gate_tables(routes, route_weights, experts, rank, pair_rank):
    gate_values = route_weights / jnp.sum(route_weights, axis=1, keepdims=True) * 2.5
    hits = routes.T[:, None, :] == experts
    gates_of = jnp.sum(jnp.where(hits, gate_values.T[:, None, :], 0.0), axis=0)
    table = jnp.concatenate([rank, gates_of.reshape(rank.shape), pair_rank], axis=1)
    count = rank.shape[0]
    return [table[0]] + [lax.ppermute(table[j], "z", ring(count, j)) for j in range(1, count)]


def layer(
    out_gate,
    in_gate,
    conv_values,
    conv_taps,
    mix_gain,
    out_proj,
    residual,
    ffn_gain,
    routes,
    route_weights,
    shared_gate,
    shared_up,
    shared_down,
    expert_gate,
    expert_up,
    expert_down,
):
    z_count, tp_count = lax.axis_size("z"), lax.axis_size(TP)
    chips = lax.axis_size(CHIPS)
    z_index, tp_index = lax.axis_index("z"), lax.axis_index(TP)
    chip_index, core_index = lax.axis_index(CHIPS), lax.axis_index("c")

    back = conv_taps.shape[0] - 1
    length = conv_values.shape[0]
    tail = in_gate[length - back :].astype(F32) * conv_values[length - back :].astype(F32)
    halo = from_behind(tail, 1)
    me = tp_index.reshape(1).astype(jnp.int32)
    seq = lax.axis_index(SEQ).reshape(1).astype(jnp.int32)
    blocks, head = filter_rows(me, out_gate, in_gate, conv_values, conv_taps, tp_count)
    blocks = mend_rows(me, seq, blocks, head, back, halo)
    pieces = exchange(blocks, TP)
    routes, _ = lax.optimization_barrier((routes, blocks[0]))
    mix_gain, _ = lax.optimization_barrier((mix_gain, pieces[1]))

    row_count, top_count = routes.shape
    capacity = max(2, 4 * row_count * top_count // (6 * z_count * chips))
    place = z_index ^ (z_index >> 1) ^ (z_index >> 2)
    later = (jnp.arange(z_count, dtype=jnp.int32) + place) & (z_count - 1)
    layers = later ^ (later >> 1)
    cores = jnp.arange(2, dtype=jnp.int32) ^ core_index
    places = jnp.arange(chips, dtype=jnp.int32) ^ chip_index
    experts = (layers[:, None, None] * chips + places) * 2 + cores[:, None]
    experts = experts.reshape(-1)[None, :, None]
    named = jnp.any(routes.T[:, None, :] == experts, axis=0)
    steps = jnp.arange(row_count, dtype=jnp.int32)
    earlier = (steps[:, None] < steps[None, :]).astype(BF16)
    rank = jnp.dot(named.astype(BF16), earlier, preferred_element_type=F32)
    rank = jnp.where(named, rank, -1.0)
    out_proj, rank = lax.optimization_barrier((out_proj, rank))
    rank = rank.reshape(z_count, 2 * chips, row_count)
    pair_rank = lax.ppermute(rank[:, chips:], "c", flips(2, 1))
    out_proj = fetch(out_proj)

    stream, normed = mix_project(me, pieces, mix_gain, out_proj, residual, ffn_gain)

    sources = gather_ring(normed, z_count)
    weights = (expert_gate, expert_up, expert_down)
    tables, results = [], []
    for j in range(z_count):
        pair = lax.ppermute(sources[j], "c", flips(2, 1))
        table = tables[j] if j else jnp.concatenate([rank[0], pair_rank[0]])
        outgoing = outgoing_rows(sources[j], pair, table, chips, capacity)
        if j == 0:
            tables = gate_tables(routes, route_weights, experts, rank, pair_rank)
        arrived = exchange(outgoing, CHIPS)
        results.append(expert_rows(arrived, 2 * chips, *weights))

    base = shared_rows(normed, stream, shared_gate, shared_up, shared_down)

    partial, short = [None] * z_count, [None] * z_count
    for j in reversed(range(z_count)):
        returned = exchange(results[j], PLANE)
        partial[j], short[j] = combine(returned, tables[j])

    if z_count == 4:

        def hop(block, distance):
            route = ring(4, distance)
            return lax.ppermute(block.astype(BF16), "z", route).astype(F32)

        back = hop(short[1], -1)
        ahead = hop(short[2], 1)
        ahead = hop(ahead + partial[3], 1)
        routed = partial[0] + back + ahead
    else:
        routed = partial[0]
        for j in range(1, z_count):
            routed = routed + lax.ppermute(short[j], "z", ring(z_count, -j))
    return (base + routed).astype(BF16)


def solution(mesh):
    sp_count, tp_count = mesh.shape["sp"], mesh.shape["tp"]
    z_count = 1 << -(-(sp_count.bit_length() - 1) // 2)
    every = SEQ + TP
    split = Mesh(
        mesh.devices.reshape(z_count, sp_count // z_count, tp_count // 2, 2), every
    )
    in_specs = (
        P(SEQ, TP),
        P(SEQ, TP),
        P(SEQ, TP),
        P(None, TP),
        P(),
        P(),
        P(every, None),
        P(),
        P(every, None),
        P(every, None),
        P(),
        P(),
        P(),
        P(every, None, None),
        P(every, None, None),
        P(every, None, None),
    )
    return jax.shard_map(
        layer, mesh=split, in_specs=in_specs, out_specs=P(every, None), check_vma=False
    )
```
